256 devices in a mesh: ep: 16 (over y, x), tp: 16 (over z, core).
Axes of the slice: x: 4, y: 4, z: 8, core: 2. Of those that a mesh axis runs over, the one named last changes fastest.
Arguments:
- q_latent: bfloat16 [16384, 512], P('ep'), may hold values from -6 to 6
- kv_latent: bfloat16 [16384, 256], P('ep'), may hold values from -6 to 6
- rope_key: bfloat16 [16384, 32], P('ep'), may hold values from -1200 to 1200
- q_gain: float32 [512], replicated, may hold values from 0.1 to 1.9
- kv_gain: float32 [256], replicated, may hold values from 0.1 to 1.9
- w_query: bfloat16 [512, 1536], P(None, 'tp'), may hold values from -0.25 to 0.25
- w_keyval: bfloat16 [256, 2048], P(None, 'tp'), may hold values from -0.375 to 0.375
- w_output: bfloat16 [1024, 2048], P(None, 'tp'), may hold values from -0.1875 to 0.1875
- moe_input: bfloat16 [8192, 2048], P('ep'), may hold values from -6 to 6
- moe_gain: float32 [2048], replicated, may hold values from 0.1 to 1.9
- routes: int32 [8192, 2], P('ep'), may hold values from 0 to 15, all different within a row; in each aligned block of 32 rows (0 to 31, 32 to 63, ...) at most 6 rows name the same one
- route_weight: float32 [8192, 2], P('ep'), may hold values from 0.25 to 2
- expert_gate: bfloat16 [16, 2048, 4096], P('ep', None, 'tp'), may hold values from -0.125 to 0.125
- expert_up: bfloat16 [16, 2048, 4096], P('ep', None, 'tp'), may hold values from -0.125 to 0.125
- expert_down: bfloat16 [16, 4096, 2048], P('ep', 'tp'), may hold values from -0.09375 to 0.09375
- shared_gate: bfloat16 [2048, 2048], P(None, 'tp'), may hold values from -0.125 to 0.125
- shared_up: bfloat16 [2048, 2048], P(None, 'tp'), may hold values from -0.125 to 0.125
- shared_down: bfloat16 [2048, 2048], P('tp'), may hold values from -0.125 to 0.125
Outputs:
- mixed: bfloat16 [16384, 2048], P('ep', 'tp')
- moe_out: bfloat16 [8192, 2048], P(('ep', 'tp'))
The draws below stay inside these ranges and needn't reach their ends.
Inputs may be any that keep to these rules, and one draw needn't show every extreme that they name: `routes`: in each aligned block of 32 rows (the rows of one device's output) no expert is named by more than 6 rows, a bound that some block reaches. Each row names 2 different experts.
All inputs are finite; a program needn't handle non-finite values.
Results may differ from the reference program's by a relative error of at most 0.023.
Values may be sent and summed in bfloat16 or wider, within the bound.
A program may use at most 128 MiB of HBM per device.

```python
import math
import jax
import jax.numpy as jnp
import numpy as np
from jax import lax

D = 2048
HEADS = 16
NOPE = 64
ROPE_DIM = 32
VDIM = 64
QLAT = 512
KVLAT = 256
TOKA_EP = 1024
TOK_A = 16384
MOE_DEV = 32
TOK_B = 8192
EXPERTS = 16
FE = 4096
FS = 2048
FE_PART = 256
FS_PART = 128
TOP = 2
CAP = 6
N_EP = 16
N_TP = 16


def draw_rope_key(key, part):
    drawn = jax.random.normal(jax.random.fold_in(key, 11), (TOK_A, ROPE_DIM), jnp.float32)
    drawn = jnp.clip(drawn, -6.0, 6.0)
    return drawn.astype(jnp.bfloat16)


def block_scale(own_key, extent, split, smallest, top_value):
    level = 1.0
    for axis_at, parts in split:
        heights = jax.random.uniform(jax.random.fold_in(jax.random.fold_in(own_key, 6), axis_at), (parts,), jnp.float32, smallest / len(split), top_value / len(split))
        level = level * jnp.repeat(jnp.exp(heights), extent[axis_at] // parts).reshape((-1,) + (1,) * (len(extent) - 1 - axis_at))
    return level


def routed_block(own_key, own, number, rows, amount, top, bound, skew):
    order = jax.random.permutation(own_key, amount)
    packed, ordinary = shares(amount, rows * top, bound, skew, True), shares(amount, rows * top, bound, skew, False)
    places = jnp.arange(amount)

    def named(lengths, offset_by):
        used = int((lengths > 0).sum())
        fixed = max(1, used // 4)
        passed = fixed + (places - fixed + offset_by * (used - fixed)) % max(1, amount - fixed)
        return jnp.zeros((amount,), jnp.int32).at[order[jnp.where(places < fixed, places, passed)]].set(jnp.asarray(lengths, jnp.int32))

    lengths = jnp.where(number % 4 == 0, named(packed, number // 4), named(ordinary, number - number // 4 - 1))
    mixed = jax.random.permutation(jax.random.fold_in(own, 3), amount)
    source_of, taker = mixed[0:amount // 2 * 2:2], mixed[1:amount // 2 * 2:2]
    room = jnp.minimum(lengths[source_of] - 1, bound - lengths[taker]) // 2
    room = jnp.where((source_of == order[0]) | (taker == order[0]) | (lengths[taker] == 0), 0, jnp.maximum(room, 0))
    passed = jax.random.randint(jax.random.fold_in(own, 4), (amount // 2,), 0, 1 << 20) % (room + 1)
    lengths = lengths.at[source_of].add(-passed).at[taker].add(passed)
    members = jnp.searchsorted(jnp.cumsum(lengths), jnp.arange(rows * top), side="right").astype(jnp.int32)
    grid = members.reshape(top, rows).T
    grid = grid[jax.random.permutation(jax.random.fold_in(own, 1), rows)]
    offset_by = jax.random.randint(jax.random.fold_in(own, 2), (rows, 1), 0, top)
    return jnp.take_along_axis(grid, (jnp.arange(top)[None, :] + offset_by) % top, axis=1)


def shares(amount, total, bound, slope, full):
    portions = [(1 << 20) // math.isqrt(rank ** slope) + 1 for rank in range(1, amount + 1)]
    largest = bound if full else min(bound, max(-(-total // amount), total * portions[0] // sum(portions)))
    least = 1 if total - largest >= amount - 1 else 0
    holding, rest = [largest] + [least] * (amount - 1), total - largest - least * (amount - 1)
    while rest > 0:
        free = [i for i in range(1, amount) if holding[i] < largest] or [i for i in range(1, amount) if holding[i] < bound]
        whole, left = sum([portions[i] for i in free]), rest
        for i in free:
            extra = min(bound - holding[i], max(1, left * portions[i] // whole), rest)
            holding[i] = holding[i] + extra
            rest = rest - extra
    return np.array(holding)


def bell_draw(key, shape, deviation, bound, pieces=(), held_as=jnp.bfloat16):
    values = jax.random.normal(key, shape, jnp.float32) * deviation
    if len(pieces) > 0:
        values = block_scale(key, shape, pieces, -0.22, 0.18) * values
    return jnp.clip(values, min=-bound, max=bound).astype(held_as)


def setup_inputs(seed: int = 0) -> dict:
    streams_of = jax.random.split(jax.random.key(seed), 19)
    q_latent = bell_draw(streams_of[0], (TOK_A, QLAT), 1.0, 6.0, ((0, 16),))
    kv_latent = bell_draw(streams_of[1], (TOK_A, KVLAT), 1.0, 6.0, ((0, 16),))
    rope_key = draw_rope_key(jax.random.fold_in(streams_of[18], 71), 0)
    q_gain = jnp.clip(1.0 + 0.18 * jax.random.normal(streams_of[3], (QLAT,), jnp.float32), 0.1, 1.9)
    kv_gain = jnp.clip(1.0 + 0.18 * jax.random.normal(streams_of[4], (KVLAT,), jnp.float32), 0.1, 1.9)
    w_query = bell_draw(streams_of[5], (QLAT, HEADS * (NOPE + ROPE_DIM)), QLAT ** -0.5, 0.25, ((1, 16),))
    w_keyval = bell_draw(streams_of[6], (KVLAT, HEADS * (NOPE + VDIM)), KVLAT ** -0.5, 0.375, ((1, 16),))
    w_output = bell_draw(streams_of[7], (HEADS * VDIM, D), (HEADS * VDIM) ** -0.5, 0.1875, ((1, 16),))
    moe_input = bell_draw(streams_of[8], (TOK_B, D), 1.0, 6.0, ((0, 16),))
    moe_gain = jnp.clip(1.0 + 0.18 * jax.random.normal(streams_of[9], (D,), jnp.float32), 0.1, 1.9)
    routes_keys = jax.random.split(jax.random.fold_in(streams_of[10], 1), TOK_B // MOE_DEV)
    routes_turns = jax.random.permutation(jax.random.fold_in(streams_of[10], 3), TOK_B // MOE_DEV)
    routes = jax.vmap(lambda own, number: routed_block(jax.random.fold_in(streams_of[10], 2), own, number, MOE_DEV, EXPERTS, TOP, CAP, 1))(routes_keys, routes_turns).reshape((TOK_B, TOP))
    route_weight = jnp.clip(0.25 + 1.75 * jax.random.uniform(streams_of[11], (TOK_B, TOP), jnp.float32) ** block_scale(streams_of[11], (TOK_B, TOP), ((0, 16),), -0.2, 0.2), 0.25, 2.0)
    expert_gate = bell_draw(streams_of[12], (EXPERTS, D, FE), D ** -0.5, 0.125, ((0, 16), (2, 16)))
    expert_up = bell_draw(streams_of[13], (EXPERTS, D, FE), D ** -0.5, 0.125, ((0, 16), (2, 16)))
    expert_down = bell_draw(streams_of[14], (EXPERTS, FE, D), FE ** -0.5, 0.09375, ((0, 16), (1, 16)))
    shared_gate = bell_draw(streams_of[15], (D, FS), D ** -0.5, 0.125, ((1, 16),))
    shared_up = bell_draw(streams_of[16], (D, FS), D ** -0.5, 0.125, ((1, 16),))
    shared_down = bell_draw(streams_of[17], (FS, D), FS ** -0.5, 0.125, ((0, 16),))
    return dict(q_latent=q_latent, kv_latent=kv_latent, rope_key=rope_key, q_gain=q_gain, kv_gain=kv_gain, w_query=w_query, w_keyval=w_keyval, w_output=w_output, moe_input=moe_input, moe_gain=moe_gain, routes=routes, route_weight=route_weight, expert_gate=expert_gate, expert_up=expert_up, expert_down=expert_down, shared_gate=shared_gate, shared_up=shared_up, shared_down=shared_down)


norm_eps = 1e-06
layer_eps = 1e-05
rotary_base = 10000.0
floor_value = -1e+30

def rms_scale(values, gain):
    widened = values.astype(jnp.float32)
    return (widened * lax.rsqrt(lax.optimization_barrier(jnp.mean(widened * widened, -1, keepdims=True)) + norm_eps) * gain).astype(jnp.bfloat16)

def layer_scale(values, gain):
    widened = values.astype(jnp.float32)
    centred = widened - lax.optimization_barrier(jnp.mean(widened, -1, keepdims=True))
    return (centred * lax.rsqrt(lax.optimization_barrier(jnp.mean(centred * centred, -1, keepdims=True)) + layer_eps) * gain).astype(jnp.bfloat16)

def rotary_tables(positions):
    halfway = ROPE_DIM // 2
    inverse = rotary_base ** (-(jnp.arange(halfway, dtype=jnp.float32) * 2.0 / ROPE_DIM))
    angles = positions.astype(jnp.float32)[:, None] * inverse[None, :]
    return (jnp.cos(angles), jnp.sin(angles))

def rotate(values, cosine_table, sine_table):
    halfway = values.shape[-1] // 2
    first_half = values[..., :halfway]
    second_half = values[..., halfway:]
    return jnp.concatenate([first_half * cosine_table - second_half * sine_table, second_half * cosine_table + first_half * sine_table], -1)

def merge_block(carried, stats):
    running_max, running_sum, running_acc = carried
    block_max, block_sum, attended = stats
    new_max = jnp.maximum(running_max, block_max)
    old_weight = jnp.exp(running_max - new_max)
    new_weight = jnp.exp(block_max - new_max)
    return (new_max, running_sum * old_weight + block_sum * new_weight, running_acc * old_weight[..., None] + attended.astype(jnp.float32) * new_weight[..., None])

def group_sum(hidden, down_weight, group_width):

    def add_group(group_index, total):
        hidden_cols = lax.dynamic_slice_in_dim(hidden, group_index * group_width, group_width, 1)
        weight_rows = lax.dynamic_slice_in_dim(down_weight, group_index * group_width, group_width, 0)
        product = jnp.dot(hidden_cols, weight_rows, preferred_element_type=jnp.float32)
        return total + lax.optimization_barrier(product.astype(jnp.bfloat16)).astype(jnp.float32)
    return lax.fori_loop(0, N_TP, add_group, jnp.zeros((hidden.shape[0], down_weight.shape[1]), jnp.float32))

def reference(q_latent, kv_latent, rope_key, q_gain, kv_gain, w_query, w_keyval, w_output, moe_input, moe_gain, routes, route_weight, expert_gate, expert_up, expert_down, shared_gate, shared_up, shared_down):
    positions = jnp.arange(TOK_A, dtype=jnp.int32)
    cosine_table, sine_table = rotary_tables(positions)
    q_normed = rms_scale(q_latent, q_gain)
    kv_normed = rms_scale(kv_latent, kv_gain)
    key_rot = rotate(rope_key.astype(jnp.float32), cosine_table, sine_table).astype(jnp.bfloat16)
    projected = jnp.dot(q_normed, w_query, preferred_element_type=jnp.float32).reshape(TOK_A, HEADS, NOPE + ROPE_DIM)
    queries = jnp.concatenate([projected[..., :NOPE], rotate(projected[..., NOPE:], cosine_table[:, None, :], sine_table[:, None, :])], -1).astype(jnp.bfloat16)
    keyvals = jnp.dot(kv_normed, w_keyval, preferred_element_type=jnp.float32).astype(jnp.bfloat16)
    keyvals = keyvals.reshape(TOK_A, HEADS, NOPE + VDIM)
    scale = float(NOPE + ROPE_DIM) ** (-0.5)

    def visit_group(group_index):
        first_row = group_index * TOKA_EP
        query_block = lax.dynamic_slice_in_dim(queries, first_row, TOKA_EP, 0).astype(jnp.float32)
        query_pos = first_row + jnp.arange(TOKA_EP, dtype=jnp.int32)

        def visit_block(block_index, carried):
            key_first = block_index * TOKA_EP
            keyval_block = lax.dynamic_slice_in_dim(keyvals, key_first, TOKA_EP, 0).astype(jnp.float32)
            rotated_block = lax.dynamic_slice_in_dim(key_rot, key_first, TOKA_EP, 0).astype(jnp.float32)
            key_pos = key_first + jnp.arange(TOKA_EP, dtype=jnp.int32)
            scores = jnp.einsum('qhd,khd->hqk', query_block[..., :NOPE], keyval_block[..., :NOPE])
            scores = (scores + jnp.einsum('qhd,kd->hqk', query_block[..., NOPE:], rotated_block)) * scale
            allowed = key_pos[None, :] <= query_pos[:, None]
            scores = jnp.where(allowed[None], scores, -jnp.inf)
            block_max = lax.optimization_barrier(jnp.max(scores, -1))
            weights = jnp.exp(scores - block_max[..., None])
            block_sum = lax.optimization_barrier(jnp.sum(weights, -1))
            rounded = lax.optimization_barrier(weights.astype(jnp.bfloat16)).astype(jnp.float32)
            attended = jnp.einsum('hqk,khd->qhd', rounded, keyval_block[..., NOPE:])
            attended = lax.optimization_barrier(attended.astype(jnp.bfloat16)).astype(jnp.float32)
            return merge_block(carried, (block_max.T, block_sum.T, attended))
        initial = (jnp.full((TOKA_EP, HEADS), floor_value, jnp.float32), jnp.zeros((TOKA_EP, HEADS), jnp.float32), jnp.zeros((TOKA_EP, HEADS, VDIM), jnp.float32))
        running_max, running_sum, running_acc = lax.fori_loop(0, group_index + 1, visit_block, initial)
        return (running_acc / running_sum[..., None]).astype(jnp.bfloat16).reshape(TOKA_EP, HEADS * VDIM)
    heads_out = lax.map(visit_group, jnp.arange(N_EP, dtype=jnp.int32)).reshape(TOK_A, HEADS * VDIM)
    mixed = jnp.dot(heads_out, w_output, preferred_element_type=jnp.float32).astype(jnp.bfloat16)
    block_total = TOK_B // MOE_DEV
    normed = layer_scale(moe_input, moe_gain)
    entries = routes.reshape(block_total, MOE_DEV * TOP)
    onehot = (entries[..., None] == jnp.arange(EXPERTS, dtype=jnp.int32)).astype(jnp.int32)
    earlier = jnp.cumsum(onehot, 1) - onehot
    rank_in = lax.optimization_barrier(jnp.sum(earlier * onehot, -1))
    block_ids = jnp.broadcast_to(jnp.arange(block_total, dtype=jnp.int32)[:, None], entries.shape)
    token_ids = (jnp.arange(TOK_B * TOP, dtype=jnp.int32) // TOP).reshape(block_total, MOE_DEV * TOP)
    table = jnp.full((EXPERTS, block_total, CAP), -1, jnp.int32).at[entries, block_ids, rank_in].set(token_ids)

    def run_expert(operands):
        slot_token, gate_weight, up_weight, down_weight = operands
        inputs = jnp.where((slot_token >= 0)[:, None], normed[jnp.maximum(slot_token, 0)], jnp.zeros((), jnp.bfloat16))
        hidden = jax.nn.silu(jnp.dot(inputs, gate_weight, preferred_element_type=jnp.float32))
        hidden = (hidden * jnp.dot(inputs, up_weight, preferred_element_type=jnp.float32)).astype(jnp.bfloat16)
        return group_sum(hidden, down_weight, FE_PART)
    expert_sums = lax.map(run_expert, (table.reshape(EXPERTS, block_total * CAP), expert_gate, expert_up, expert_down))
    slot_of = ((entries * block_total + block_ids) * CAP + rank_in).reshape(TOK_B, TOP)
    picked = expert_sums.reshape(EXPERTS * block_total * CAP, D)[slot_of]
    routed = lax.optimization_barrier(jnp.sum(route_weight[..., None] * picked, 1))
    shared_hidden = jax.nn.silu(jnp.dot(normed, shared_gate, preferred_element_type=jnp.float32))
    shared_hidden = (shared_hidden * jnp.dot(normed, shared_up, preferred_element_type=jnp.float32)).astype(jnp.bfloat16)
    shared_total = group_sum(shared_hidden, shared_down, FS_PART)
    moe_out = (routed + shared_total).astype(jnp.bfloat16)
    return (mixed, moe_out)
```

```python
import functools

import jax
import jax.numpy as jnp
from jax import lax
from jax.experimental import pallas as pl
from jax.experimental.pallas import tpu as pltpu
from jax.sharding import PartitionSpec as P

NOPE = 64
ROPE_DIM = 32
VDIM = 64
MOE_DEV = 32
CAP = 6
PAD = 8

norm_eps = 1e-06
layer_eps = 1e-05
rotary_base = 10000.0
floor_value = -1e30
QTILE = 256
LOG2E = 1.4426950408889634


def rms_scale(values, gain):
    widened = values.astype(jnp.float32)
    return (
        widened * lax.rsqrt(jnp.mean(widened * widened, -1, keepdims=True) + norm_eps) * gain
    ).astype(jnp.bfloat16)


def layer_scale(values, gain):
    widened = values.astype(jnp.float32)
    centred = widened - jnp.mean(widened, -1, keepdims=True)
    return (
        centred * lax.rsqrt(jnp.mean(centred * centred, -1, keepdims=True) + layer_eps) * gain
    ).astype(jnp.bfloat16)


def rotary_tables(positions):
    halfway = ROPE_DIM // 2
    inverse = rotary_base ** (-(jnp.arange(halfway, dtype=jnp.float32) * 2.0 / ROPE_DIM))
    angles = positions.astype(jnp.float32)[None, :] * inverse[:, None]
    return (jnp.cos(angles), jnp.sin(angles))


def rotate_rows(values, cosine_table, sine_table):
    halfway = values.shape[0] // 2
    first_half = values[:halfway]
    second_half = values[halfway:]
    return jnp.concatenate(
        [
            first_half * cosine_table - second_half * sine_table,
            second_half * cosine_table + first_half * sine_table,
        ],
        0,
    )


def attention_kernel(own_ref, q_ref, kv_ref, out_ref, m_ref, l_ref, acc_ref):
    block = pl.program_id(0)
    own = own_ref[0]
    width = q_ref.shape[1]
    score_rows = NOPE + ROPE_DIM
    scale = float(score_rows) ** (-0.5) * LOG2E

    @pl.when(block == 0)
    def _():
        m_ref[...] = jnp.full_like(m_ref, floor_value)
        l_ref[...] = jnp.zeros_like(l_ref)
        acc_ref[...] = jnp.zeros_like(acc_ref)

    def visit(tile, key_count, masked):
        cols = pl.ds(tile * QTILE, QTILE)
        scores = lax.dot_general(
            kv_ref[0:score_rows, 0:key_count],
            q_ref[:, cols],
            (((0,), (0,)), ((), ())),
            preferred_element_type=jnp.float32,
        )
        if masked:
            key_at = lax.broadcasted_iota(jnp.int32, scores.shape, 0)
            query_at = tile * QTILE + lax.broadcasted_iota(jnp.int32, scores.shape, 1)
            scores = jnp.where(key_at <= query_at, scores, floor_value)
        old_max = m_ref[:, cols]
        new_max = jnp.maximum(old_max, jnp.max(scores, 0, keepdims=True))
        weights = jnp.exp2((scores - new_max) * scale)
        fade = jnp.exp2((old_max - new_max) * scale)
        l_ref[:, cols] = l_ref[:, cols] * fade + jnp.sum(weights, 0, keepdims=True)
        attended = jnp.dot(
            kv_ref[score_rows:, 0:key_count],
            weights.astype(jnp.bfloat16),
            preferred_element_type=jnp.float32,
        )
        acc_ref[:, cols] = acc_ref[:, cols] * fade + attended
        m_ref[:, cols] = new_max

    @pl.when(block < own)
    def _():
        for tile in range(width // QTILE):
            visit(tile, width, False)

    @pl.when(block == own)
    def _():
        for tile in range(width // QTILE):
            visit(tile, (tile + 1) * QTILE, True)
        out_ref[...] = (acc_ref[...] / l_ref[...]).astype(out_ref.dtype)


def attention(own_index, queries, keyvals):
    rows, width = queries.shape
    kv_rows = rows + VDIM
    blocks = keyvals.shape[0] // kv_rows
    return pl.pallas_call(
        attention_kernel,
        out_shape=jax.ShapeDtypeStruct((VDIM, width), jnp.bfloat16),
        grid_spec=pltpu.PrefetchScalarGridSpec(
            num_scalar_prefetch=1,
            grid=(blocks,),
            in_specs=[
                pl.BlockSpec((rows, width), lambda i, own: (0, 0)),
                pl.BlockSpec((kv_rows, width), lambda i, own: (jnp.minimum(i, own[0]), 0)),
            ],
            out_specs=pl.BlockSpec((VDIM, width), lambda i, own: (0, 0)),
            scratch_shapes=[
                pltpu.VMEM((1, width), jnp.float32),
                pltpu.VMEM((1, width), jnp.float32),
                pltpu.VMEM((VDIM, width), jnp.float32),
            ],
        ),
        compiler_params=pltpu.CompilerParams(
            dimension_semantics=("arbitrary",), vmem_limit_bytes=40 << 20
        ),
        cost_estimate=pl.CostEstimate(
            flops=20_000_000_000, bytes_accessed=5_000_000, transcendentals=8_000_000
        ),
        name="attention",
    )(own_index.reshape(1).astype(jnp.int32), queries, keyvals)


def body(
    q_latent,
    kv_latent,
    rope_key,
    q_gain,
    kv_gain,
    w_query,
    w_keyval,
    w_output,
    moe_input,
    moe_gain,
    routes,
    route_weight,
    expert_gate,
    expert_up,
    expert_down,
    shared_gate,
    shared_up,
    shared_down,
):
    f32, bf16 = jnp.float32, jnp.bfloat16
    row_count = q_latent.shape[0]
    own_index = lax.axis_index("ep")
    ep_count = lax.axis_size("ep")
    tp_count = lax.axis_size("tp")
    width = moe_input.shape[1]
    top_count = routes.shape[1]

    own_block = lax.axis_index("tp")
    own_input = lax.dynamic_slice_in_dim(moe_input, own_block * MOE_DEV, MOE_DEV, 0)
    own_normed = layer_scale(own_input, moe_gain)
    own_routes = lax.dynamic_slice_in_dim(routes, own_block * MOE_DEV, MOE_DEV, 0)
    own_weight = lax.dynamic_slice_in_dim(route_weight, own_block * MOE_DEV, MOE_DEV, 0)
    experts = jnp.arange(ep_count, dtype=jnp.int32)
    named = (own_routes[:, :, None] == experts).astype(f32)
    in_row = jnp.sum(named, 1)
    token_at = jnp.arange(MOE_DEV)
    before = (token_at[None, :] < token_at[:, None]).astype(f32)
    rank = jnp.dot(before, in_row, preferred_element_type=f32)
    slot_at = jnp.arange(PAD, dtype=f32)
    taken = jnp.where(
        (in_row[:, :, None] > 0) & (rank[:, :, None] == slot_at), 1.0, 0.0
    )
    weight_of = jnp.sum(named * own_weight[:, :, None], 1)
    combine = (taken * weight_of[:, :, None]).reshape(MOE_DEV, ep_count * PAD)
    select = taken.reshape(MOE_DEV, ep_count * PAD).astype(bf16)
    outgoing = lax.dot_general(
        select, own_normed, (((0,), (0,)), ((), ())), preferred_element_type=f32
    ).astype(bf16)
    arrived = lax.all_to_all(outgoing, "ep", split_axis=0, concat_axis=0, tiled=True)
    squeeze = (
        jnp.arange(ep_count * PAD)[None, :]
        == (jnp.arange(ep_count * CAP) // CAP * PAD + jnp.arange(ep_count * CAP) % CAP)[:, None]
    ).astype(bf16)
    compact = jnp.dot(squeeze, arrived, preferred_element_type=f32).astype(bf16)
    inputs = lax.all_gather(compact, "tp", axis=0, tiled=True)

    positions = own_index * row_count + jnp.arange(row_count, dtype=jnp.int32)
    cosine_table, sine_table = rotary_tables(positions)
    q_normed = rms_scale(q_latent, q_gain)
    kv_normed = rms_scale(kv_latent, kv_gain)
    key_rotated = rotate_rows(rope_key.T.astype(f32), cosine_table, sine_table).astype(bf16)
    projected = lax.dot_general(
        w_query, q_normed, (((0,), (1,)), ((), ())), preferred_element_type=f32
    )
    queries = jnp.concatenate(
        [projected[:NOPE], rotate_rows(projected[NOPE:], cosine_table, sine_table)], 0
    ).astype(bf16)
    expanded = lax.dot_general(
        w_keyval, kv_normed, (((0,), (1,)), ((), ())), preferred_element_type=f32
    ).astype(bf16)
    own_keyvals = jnp.concatenate([expanded[:NOPE], key_rotated, expanded[NOPE:]], 0)
    keyvals = lax.all_gather(own_keyvals, "ep", axis=0, tiled=True)

    heads_own = attention(own_index, queries, keyvals)
    heads_out = lax.all_gather(heads_own, "tp", axis=0, tiled=True)
    mixed = lax.dot_general(
        heads_out, w_output, (((0,), (0,)), ((), ())), preferred_element_type=f32
    ).astype(bf16)

    normed = layer_scale(moe_input, moe_gain)
    shared_hidden = jax.nn.silu(jnp.dot(normed, shared_gate, preferred_element_type=f32))
    shared_hidden = (shared_hidden * jnp.dot(normed, shared_up, preferred_element_type=f32)).astype(
        bf16
    )
    shared_part = jnp.dot(shared_hidden, shared_down, preferred_element_type=f32).astype(bf16)

    hidden = jax.nn.silu(jnp.dot(inputs, expert_gate[0], preferred_element_type=f32))
    hidden = (hidden * jnp.dot(inputs, expert_up[0], preferred_element_type=f32)).astype(bf16)
    routed_part = jnp.dot(hidden, expert_down[0], preferred_element_type=f32).astype(bf16)
    routed_total = lax.psum_scatter(routed_part, "tp", scatter_dimension=0, tiled=True)
    shared_total = lax.psum_scatter(shared_part, "tp", scatter_dimension=0, tiled=True)
    spread = lax.dot_general(
        squeeze, routed_total, (((0,), (0,)), ((), ())), preferred_element_type=f32
    ).astype(bf16)
    returned = lax.all_to_all(spread, "ep", split_axis=0, concat_axis=0, tiled=True)
    combine_high = combine.astype(bf16)
    combine_low = (combine - combine_high.astype(f32)).astype(bf16)
    moe_out = (
        jnp.dot(combine_high, returned, preferred_element_type=f32)
        + jnp.dot(combine_low, returned, preferred_element_type=f32)
        + shared_total.astype(f32)
    ).astype(bf16)
    return (mixed, moe_out)


def solution(mesh):
    in_specs = (
        P("ep", None),
        P("ep", None),
        P("ep", None),
        P(),
        P(),
        P(None, "tp"),
        P(None, "tp"),
        P(None, "tp"),
        P("ep", None),
        P(),
        P("ep", None),
        P("ep", None),
        P("ep", None, "tp"),
        P("ep", None, "tp"),
        P("ep", "tp", None),
        P(None, "tp"),
        P(None, "tp"),
        P("tp", None),
    )
    out_specs = (P("ep", "tp"), P(("ep", "tp"), None))
    return jax.shard_map(body, mesh=mesh, in_specs=in_specs, out_specs=out_specs, check_vma=False)
```

```python
import functools

import jax
import jax.numpy as jnp
from jax import lax
from jax.experimental import pallas as pl
from jax.experimental.pallas import tpu as pltpu
from jax.sharding import PartitionSpec as P

NOPE = 64
ROPE_DIM = 32
VDIM = 64
MOE_DEV = 32
CAP = 6
PAD = 8

norm_eps = 1e-06
layer_eps = 1e-05
rotary_base = 10000.0
floor_value = -1e30
QTILE = 256
LOG2E = 1.4426950408889634


def rms_scale(values, gain):
    widened = values.astype(jnp.float32)
    return (
        widened * lax.rsqrt(jnp.mean(widened * widened, -1, keepdims=True) + norm_eps) * gain
    ).astype(jnp.bfloat16)


def layer_scale(values, gain):
    widened = values.astype(jnp.float32)
    centred = widened - jnp.mean(widened, -1, keepdims=True)
    return (
        centred * lax.rsqrt(jnp.mean(centred * centred, -1, keepdims=True) + layer_eps) * gain
    ).astype(jnp.bfloat16)


def rotary_tables(positions):
    halfway = ROPE_DIM // 2
    inverse = rotary_base ** (-(jnp.arange(halfway, dtype=jnp.float32) * 2.0 / ROPE_DIM))
    angles = positions.astype(jnp.float32)[None, :] * inverse[:, None]
    return (jnp.cos(angles), jnp.sin(angles))


def rotate_rows(values, cosine_table, sine_table):
    halfway = values.shape[0] // 2
    first_half = values[:halfway]
    second_half = values[halfway:]
    return jnp.concatenate(
        [
            first_half * cosine_table - second_half * sine_table,
            second_half * cosine_table + first_half * sine_table,
        ],
        0,
    )


MESH = pl.DeviceIdType.MESH


def fused_kernel(
    ep_count,
    z_count,
    outgoing_ref,
    q_ref,
    own_kv_ref,
    normed_ref,
    gate_ref,
    up_ref,
    down_ref,
    sgate_ref,
    sup_ref,
    sdown_ref,
    chigh_ref,
    clow_ref,
    wout_ref,
    mixed_ref,
    moe_ref,
    recv_a,
    buf_x,
    buf_p,
    recv_d,
    buf_s,
    recv_r,
    final,
    kv,
    heads,
    send_b,
    recv_b,
    q_t,
    m_t,
    l_t,
    acc_t,
    a_send,
    a_recv,
    k_send,
    k_recv,
    x_send,
    x_recv,
    xd_send,
    xd_recv,
    p_send,
    p_recv,
    r_send,
    r_recv,
    h_send,
    h_recv,
    hd_send,
    hd_recv,
    b_send,
    b_recv,
):
    f32, bf16 = jnp.float32, jnp.bfloat16
    ep = lax.axis_index("ep")
    tp = lax.axis_index("tp")
    z = lax.div(tp, 2)
    core = lax.rem(tp, 2)
    other = 1 - core
    half_ring = z_count // 2
    steps = half_ring - 1
    slots = ep_count * CAP
    rows = slots + MOE_DEV
    width = normed_ref.shape[1]
    score_rows = NOPE + ROPE_DIM
    length = q_ref.shape[1]
    tiles = length // QTILE
    scale = float(score_rows) ** (-0.5) * LOG2E
    partner = {"tp": z * 2 + other}
    x_half = slots // 2
    r_half = rows // 2
    r_cols = width // 2
    h_half = VDIM // 2

    def around(offset):
        return lax.rem(z + offset + 2 * z_count, z_count)

    def at_z(offset):
        return {"tp": around(offset) * 2 + core}

    def at_ep(offset):
        return {"ep": lax.rem(ep + offset + ep_count, ep_count)}

    def remote(src, dst, send, recv, device):
        return pltpu.make_async_remote_copy(
            src_ref=src, dst_ref=dst, send_sem=send, recv_sem=recv,
            device_id=device, device_id_type=MESH,
        )

    def loop(low, high, step):
        def run(index, carry):
            step(index)
            return carry

        lax.fori_loop(low, high, run, 0)

    barrier = pltpu.get_barrier_semaphore()
    loop(1, ep_count, lambda d: pl.semaphore_signal(
        barrier, inc=1, device_id=at_ep(d), device_id_type=MESH))
    for device in (at_z(1), at_z(-1), partner):
        pl.semaphore_signal(barrier, inc=1, device_id=device, device_id_type=MESH)
    pl.semaphore_wait(barrier, ep_count + 2)

    def a_copy(d):
        there = lax.rem(ep + d, ep_count)
        return remote(outgoing_ref.at[there], recv_a.at[ep], a_send.at[d], a_recv.at[d], at_ep(d))

    def a_arrival(d):
        source = lax.rem(ep - d + ep_count, ep_count)
        return remote(outgoing_ref.at[ep], recv_a.at[source], a_send.at[d], a_recv.at[d], at_ep(d))

    def k_copy(d):
        return remote(own_kv_ref, kv.at[ep], k_send.at[d], k_recv.at[d], at_ep(d))

    def k_arrival(d):
        source = lax.rem(ep - d + ep_count, ep_count)
        return remote(own_kv_ref, kv.at[source], k_send.at[d], k_recv.at[d], at_ep(d))

    def guarded(test, act):
        @pl.when(test)
        def _():
            act()

    loop(1, ep_count, lambda d: a_copy(d).start())
    loop(1, ep_count, lambda d: guarded(ep + d < ep_count, lambda: k_copy(d).start()))
    recv_a[ep] = outgoing_ref[ep]

    def shared_rows(first, count):
        x = normed_ref[pl.ds(first * count * 2 * MOE_DEV, count * 2 * MOE_DEV), :]
        hidden = jax.nn.silu(jnp.dot(x, sgate_ref[...], preferred_element_type=f32))
        hidden = (hidden * jnp.dot(x, sup_ref[...], preferred_element_type=f32)).astype(bf16)
        part = jnp.dot(hidden, sdown_ref[...], preferred_element_type=f32).astype(bf16)
        for at in range(count):
            for side in range(2):
                begin = (at * 2 + side) * MOE_DEV
                buf_p[first * count + at, side, slots:rows, :] = part[begin : begin + MOE_DEV]

    per_call = 2
    loop(0, z_count // per_call, lambda first: shared_rows(first, per_call))

    for tile in range(tiles):
        q_t[tile] = q_ref[:, tile * QTILE : (tile + 1) * QTILE]
    m_t[...] = jnp.full_like(m_t, floor_value)
    l_t[...] = jnp.zeros_like(l_t)
    acc_t[...] = jnp.zeros_like(acc_t)

    def squeeze_rows(shape, slot_dim):
        slot = lax.broadcasted_iota(jnp.int32, shape, slot_dim)
        place = lax.broadcasted_iota(jnp.int32, shape, 1 - slot_dim)
        return jnp.where(
            place == lax.div(slot, CAP) * PAD + lax.rem(slot, CAP), 1.0, 0.0
        ).astype(bf16)

    loop(1, ep_count, lambda d: a_arrival(d).wait_recv())
    arrived = recv_a[...].astype(f32).reshape(ep_count * PAD, width).astype(bf16)
    buf_x[z, core] = jnp.dot(
        squeeze_rows((slots, ep_count * PAD), 0), arrived, preferred_element_type=f32
    ).astype(bf16)

    def ring_copy(buf, send, recv, size, side, step, half, origin):
        part = pl.ds(half * size, size)
        return remote(
            buf.at[origin, core, part], buf.at[origin, core, part],
            send.at[side, step, half], recv.at[side, step, half], at_z(1 - 2 * side),
        )

    def hand_copy(buf, send, recv, size, offset, half, whose):
        part = pl.ds(half * size, size)
        here = buf.at[around(offset), whose, part]
        return remote(here, here, send.at[offset, half], recv.at[offset, half], partner)

    def x_ring(side, step, half, origin):
        return ring_copy(buf_x, x_send, x_recv, x_half, side, step, half, origin)

    def x_hand(offset, half, whose):
        return hand_copy(buf_x, xd_send, xd_recv, x_half, offset, half, whose)

    def h_ring(side, step, half, origin):
        return ring_copy(heads, h_send, h_recv, h_half, side, step, half, origin)

    def h_hand(offset, half, whose):
        return hand_copy(heads, hd_send, hd_recv, h_half, offset, half, whose)

    def offset_of(side, step):
        return step if side else z_count - step

    def begin_gather(ring, hand):
        for half in range(2):
            for side in range(2):
                ring(side, 1, half, z).start()
            hand(0, half, core).start()

    def pass_on(ring, hand, step):
        for half in range(2):
            for side in range(2):
                offset = offset_of(side, step)
                origin = around(offset)
                ring(side, step, half, origin).wait_recv()
                if half == side:
                    ring(side, step + 1, half, origin).start()
                else:
                    guarded(step < steps, lambda: ring(side, step + 1, half, origin).start())
                hand(offset, half, core).start()

    def pass_last(ring, hand):
        origin = around(half_ring)
        for side in range(2):
            ring(side, half_ring, side, origin).wait_recv()
            hand(half_ring, side, core).start()

    def take_hand(hand, offset):
        for half in range(2):
            hand(offset, half, other).wait_recv()

    def p_copy(offset):
        at = around(offset)
        return remote(buf_p.at[at, other], recv_d.at[at], p_send.at[offset], p_recv.at[offset], partner)

    def expert(offset):
        at = around(offset)
        x = buf_x[at].reshape(2 * slots, width)
        hidden = jax.nn.silu(jnp.dot(x, gate_ref[...], preferred_element_type=f32))
        hidden = (hidden * jnp.dot(x, up_ref[...], preferred_element_type=f32)).astype(bf16)
        part = jnp.dot(hidden, down_ref[...], preferred_element_type=f32).astype(bf16)
        for side in range(2):
            buf_p[at, side, 0:slots, :] = part[side * slots : (side + 1) * slots]
        p_copy(offset).start()

    def pair_sum(offset):
        at = around(offset)
        p_copy(offset).wait_recv()
        for half in range(2):
            for side in range(2):
                part = (slice(half * r_half, (half + 1) * r_half), slice(side * r_cols, (side + 1) * r_cols))
                buf_s[at, side, half] = (
                    buf_p[(at, core) + part].astype(f32) + recv_d[(at,) + part].astype(f32)
                ).astype(bf16)

    def visit(block, tile, key_count, masked):
        scores = lax.dot_general(
            block[0:score_rows, 0:key_count],
            q_t[tile],
            (((0,), (0,)), ((), ())),
            preferred_element_type=f32,
        )
        if masked:
            key_at = lax.broadcasted_iota(jnp.int32, scores.shape, 0)
            query_at = tile * QTILE + lax.broadcasted_iota(jnp.int32, scores.shape, 1)
            scores = jnp.where(key_at <= query_at, scores, floor_value)
        old_max = m_t[tile]
        new_max = jnp.maximum(old_max, jnp.max(scores, 0, keepdims=True))
        weights = jnp.exp2((scores - new_max) * scale)
        fade = jnp.exp2((old_max - new_max) * scale)
        l_t[tile] = l_t[tile] * fade + jnp.sum(weights, 0, keepdims=True)
        attended = jnp.dot(
            block[score_rows:, 0:key_count], weights.astype(bf16), preferred_element_type=f32
        )
        acc_t[tile] = acc_t[tile] * fade + attended
        m_t[tile] = new_max

    def earlier_block(d):
        def act():
            k_arrival(d).wait_recv()
            for tile in range(tiles):
                visit(kv.at[ep - d], tile, length, False)

        guarded(d <= ep, act)

    early = 2 * steps

    def part_block(unit):
        d = early + 1 + lax.div(unit, 2)
        which = lax.rem(unit, 2)
        guarded(which == 0, lambda: k_arrival(d).wait_recv())
        for tile in range(tiles // 2):
            visit(kv.at[ep - d], which * (tiles // 2) + tile, length, False)

    begin_gather(x_ring, x_hand)
    for tile in range(tiles):
        visit(own_kv_ref, tile, (tile + 1) * QTILE, True)
    take_hand(x_hand, 0)
    expert(0)

    def gather_step(step):
        pass_on(x_ring, x_hand, step)
        for side in range(2):
            take_hand(x_hand, offset_of(side, step))
        loop(0, 2, lambda side: expert(lax.rem(step * (2 * side - 1) + z_count, z_count)))
        loop(2 * step - 1, 2 * step + 1, earlier_block)
        loop(0, 2, lambda side: pair_sum(lax.rem(step * (2 * side - 1) + z_count, z_count)))

    loop(1, half_ring, gather_step)
    pass_last(x_ring, x_hand)

    def r_copy(step, side, half, chunk):
        return remote(
            buf_s.at[chunk, side, half], recv_r.at[step, side, half],
            r_send.at[step, side, half], r_recv.at[step, side, half], at_z(1 - 2 * side),
        )

    for half in range(2):
        for side in range(2):
            r_copy(0, side, half, around(2 * side - 1)).start()
    pair_sum(0)
    take_hand(x_hand, half_ring)
    expert(half_ring)
    pair_sum(half_ring)

    events = 4 * (z_count - 2)
    units = 2 * jnp.maximum(ep - early, 0)

    def sum_event(event):
        step = lax.div(event, 4) + 1
        side = lax.rem(event, 2)
        half = lax.div(lax.rem(event, 4), 2)
        chunk = around((step + 1) * (2 * side - 1))
        r_copy(step - 1, side, half, chunk).wait_recv()
        buf_s[chunk, side, half] = (
            buf_s[chunk, side, half].astype(f32) + recv_r[step - 1, side, half].astype(f32)
        ).astype(bf16)
        r_copy(step, side, half, chunk).start()
        loop(lax.div(event * units, events), lax.div((event + 1) * units, events), part_block)

    loop(0, events, sum_event)

    for tile in range(tiles):
        heads[z, core, :, tile * QTILE : (tile + 1) * QTILE] = (acc_t[tile] / l_t[tile]).astype(bf16)
    begin_gather(h_ring, h_hand)

    for half in range(2):
        for side in range(2):
            r_copy(z_count - 2, side, half, z).wait_recv()
            final[half * r_half : (half + 1) * r_half, side * r_cols : (side + 1) * r_cols] = (
                buf_s[z, side, half].astype(f32) + recv_r[z_count - 2, side, half].astype(f32)
            )

    spread = jnp.dot(
        squeeze_rows((ep_count * PAD, slots), 1),
        final[0:slots, :].astype(bf16),
        preferred_element_type=f32,
    )
    send_b[...] = spread.reshape(ep_count, PAD, width).astype(bf16)

    def b_copy(d):
        there = lax.rem(ep + d, ep_count)
        return remote(send_b.at[there], recv_b.at[ep], b_send.at[d], b_recv.at[d], at_ep(d))

    def b_arrival(d):
        source = lax.rem(ep - d + ep_count, ep_count)
        return remote(send_b.at[ep], recv_b.at[source], b_send.at[d], b_recv.at[d], at_ep(d))

    loop(1, ep_count, lambda d: b_copy(d).start())
    recv_b[ep] = send_b[ep]

    loop(1, half_ring, lambda step: pass_on(h_ring, h_hand, step))
    pass_last(h_ring, h_hand)

    loop(1, ep_count, lambda d: b_arrival(d).wait_recv())
    returned = recv_b[...].astype(f32).reshape(ep_count * PAD, width).astype(bf16)
    moe_ref[...] = (
        jnp.dot(chigh_ref[...], returned, preferred_element_type=f32)
        + jnp.dot(clow_ref[...], returned, preferred_element_type=f32)
        + final[slots:rows, :]
    ).astype(bf16)

    loop(0, z_count, lambda offset: take_hand(h_hand, offset))
    mixed_ref[...] = lax.dot_general(
        heads[...].reshape(2 * z_count * VDIM, length),
        wout_ref[...],
        (((0,), (0,)), ((), ())),
        preferred_element_type=f32,
    ).astype(bf16)

    loop(1, ep_count, lambda d: a_copy(d).wait_send())
    loop(1, ep_count, lambda d: b_copy(d).wait_send())
    loop(1, ep_count, lambda d: guarded(ep + d < ep_count, lambda: k_copy(d).wait_send()))

    def left(step):
        for half in range(2):
            for side in range(2):
                x_ring(side, step, half, z).wait_send()
                h_ring(side, step, half, z).wait_send()

    loop(1, half_ring, left)
    for side in range(2):
        x_ring(side, half_ring, side, z).wait_send()
        h_ring(side, half_ring, side, z).wait_send()

    def handed(offset):
        for half in range(2):
            x_hand(offset, half, core).wait_send()
            h_hand(offset, half, core).wait_send()
        p_copy(offset).wait_send()

    loop(0, z_count, handed)

    def summed(step):
        for half in range(2):
            for side in range(2):
                r_copy(step, side, half, z).wait_send()

    loop(0, z_count - 1, summed)


def fused(ep_count, tp_count, width, operands):
    f32, bf16 = jnp.float32, jnp.bfloat16
    z_count = tp_count // 2
    half_ring = z_count // 2
    slots = ep_count * CAP
    rows = slots + MOE_DEV
    score_rows, length = operands[1].shape
    tiles = length // QTILE
    dma = pltpu.SemaphoreType.DMA
    vmem = pltpu.VMEM
    return pl.pallas_call(
        functools.partial(fused_kernel, ep_count, z_count),
        out_shape=(
            jax.ShapeDtypeStruct((length, operands[-1].shape[1]), bf16),
            jax.ShapeDtypeStruct((MOE_DEV, width), bf16),
        ),
        in_specs=[pl.BlockSpec(memory_space=pltpu.VMEM)] * len(operands),
        out_specs=(pl.BlockSpec(memory_space=pltpu.VMEM),) * 2,
        scratch_shapes=[
            vmem((ep_count, PAD, width), bf16),
            vmem((z_count, 2, slots, width), bf16),
            vmem((z_count, 2, rows, width), bf16),
            vmem((z_count, rows, width), bf16),
            vmem((z_count, 2, 2, rows // 2, width // 2), bf16),
            vmem((z_count - 1, 2, 2, rows // 2, width // 2), bf16),
            vmem((rows, width), f32),
            vmem((ep_count, score_rows + VDIM, length), bf16),
            vmem((z_count, 2, VDIM, length), bf16),
            vmem((ep_count, PAD, width), bf16),
            vmem((ep_count, PAD, width), bf16),
            vmem((tiles, score_rows, QTILE), bf16),
            vmem((tiles, 1, QTILE), f32),
            vmem((tiles, 1, QTILE), f32),
            vmem((tiles, VDIM, QTILE), f32),
            dma((ep_count,)),
            dma((ep_count,)),
            dma((ep_count,)),
            dma((ep_count,)),
            dma((2, half_ring + 1, 2)),
            dma((2, half_ring + 1, 2)),
            dma((z_count, 2)),
            dma((z_count, 2)),
            dma((z_count,)),
            dma((z_count,)),
            dma((z_count - 1, 2, 2)),
            dma((z_count - 1, 2, 2)),
            dma((2, half_ring + 1, 2)),
            dma((2, half_ring + 1, 2)),
            dma((z_count, 2)),
            dma((z_count, 2)),
            dma((ep_count,)),
            dma((ep_count,)),
        ],
        compiler_params=pltpu.CompilerParams(
            collective_id=0, has_side_effects=True, vmem_limit_bytes=62 << 20
        ),
        name="fused",
    )(*operands)


def body(
    q_latent,
    kv_latent,
    rope_key,
    q_gain,
    kv_gain,
    w_query,
    w_keyval,
    w_output,
    moe_input,
    moe_gain,
    routes,
    route_weight,
    expert_gate,
    expert_up,
    expert_down,
    shared_gate,
    shared_up,
    shared_down,
):
    f32, bf16 = jnp.float32, jnp.bfloat16
    row_count = q_latent.shape[0]
    own_index = lax.axis_index("ep")
    ep_count = lax.axis_size("ep")
    tp_count = lax.axis_size("tp")
    width = moe_input.shape[1]
    top_count = routes.shape[1]

    own_block = lax.axis_index("tp")
    own_input = lax.dynamic_slice_in_dim(moe_input, own_block * MOE_DEV, MOE_DEV, 0)
    own_normed = layer_scale(own_input, moe_gain)
    own_routes = lax.dynamic_slice_in_dim(routes, own_block * MOE_DEV, MOE_DEV, 0)
    own_weight = lax.dynamic_slice_in_dim(route_weight, own_block * MOE_DEV, MOE_DEV, 0)
    experts = jnp.arange(ep_count, dtype=jnp.int32)
    named = (own_routes[:, :, None] == experts).astype(f32)
    in_row = jnp.sum(named, 1)
    token_at = jnp.arange(MOE_DEV)
    before = (token_at[None, :] < token_at[:, None]).astype(f32)
    rank = jnp.dot(before, in_row, preferred_element_type=f32)
    slot_at = jnp.arange(PAD, dtype=f32)
    taken = jnp.where(
        (in_row[:, :, None] > 0) & (rank[:, :, None] == slot_at), 1.0, 0.0
    )
    weight_of = jnp.sum(named * own_weight[:, :, None], 1)
    combine = (taken * weight_of[:, :, None]).reshape(MOE_DEV, ep_count * PAD)
    select = taken.reshape(MOE_DEV, ep_count * PAD).astype(bf16)
    outgoing = (
        lax.dot_general(select, own_normed, (((0,), (0,)), ((), ())), preferred_element_type=f32)
        .astype(bf16)
        .reshape(ep_count, PAD, width)
    )
    positions = own_index * row_count + jnp.arange(row_count, dtype=jnp.int32)
    cosine_table, sine_table = rotary_tables(positions)
    q_normed = rms_scale(q_latent, q_gain)
    kv_normed = rms_scale(kv_latent, kv_gain)
    key_rotated = rotate_rows(rope_key.T.astype(f32), cosine_table, sine_table).astype(bf16)
    projected = lax.dot_general(
        w_query, q_normed, (((0,), (1,)), ((), ())), preferred_element_type=f32
    )
    queries = jnp.concatenate(
        [projected[:NOPE], rotate_rows(projected[NOPE:], cosine_table, sine_table)], 0
    ).astype(bf16)
    expanded = lax.dot_general(
        w_keyval, kv_normed, (((0,), (1,)), ((), ())), preferred_element_type=f32
    ).astype(bf16)
    own_keyvals = jnp.concatenate([expanded[:NOPE], key_rotated, expanded[NOPE:]], 0)
    normed = layer_scale(moe_input, moe_gain)
    combine_high = combine.astype(bf16)
    combine_low = (combine - combine_high.astype(f32)).astype(bf16)
    mixed, moe_out = fused(
        ep_count,
        tp_count,
        width,
        (
            outgoing,
            queries,
            own_keyvals,
            normed,
            expert_gate[0],
            expert_up[0],
            expert_down[0],
            shared_gate,
            shared_up,
            shared_down,
            combine_high,
            combine_low,
            w_output,
        ),
    )
    return (mixed, moe_out)


def solution(mesh):
    in_specs = (
        P("ep", None),
        P("ep", None),
        P("ep", None),
        P(),
        P(),
        P(None, "tp"),
        P(None, "tp"),
        P(None, "tp"),
        P("ep", None),
        P(),
        P("ep", None),
        P("ep", None),
        P("ep", None, "tp"),
        P("ep", None, "tp"),
        P("ep", "tp", None),
        P(None, "tp"),
        P(None, "tp"),
        P("tp", None),
    )
    out_specs = (P("ep", "tp"), P(("ep", "tp"), None))
    return jax.shard_map(body, mesh=mesh, in_specs=in_specs, out_specs=out_specs, check_vma=False)
```

```python
import functools

import jax
import jax.numpy as jnp
from jax import lax
from jax.experimental import pallas as pl
from jax.experimental.pallas import tpu as pltpu
from jax.sharding import PartitionSpec as P

NOPE = 64
ROPE_DIM = 32
VDIM = 64
MOE_DEV = 32
CAP = 6
PAD = 8

norm_eps = 1e-06
layer_eps = 1e-05
rotary_base = 10000.0
floor_value = -1e30
QTILE = 256
LOG2E = 1.4426950408889634


def rms_scale(values, gain):
    widened = values.astype(jnp.float32)
    return (
        widened * lax.rsqrt(jnp.mean(widened * widened, -1, keepdims=True) + norm_eps) * gain
    ).astype(jnp.bfloat16)


def layer_scale(values, gain):
    widened = values.astype(jnp.float32)
    centred = widened - jnp.mean(widened, -1, keepdims=True)
    return (
        centred * lax.rsqrt(jnp.mean(centred * centred, -1, keepdims=True) + layer_eps) * gain
    ).astype(jnp.bfloat16)


def rotary_tables(positions):
    halfway = ROPE_DIM // 2
    inverse = rotary_base ** (-(jnp.arange(halfway, dtype=jnp.float32) * 2.0 / ROPE_DIM))
    angles = positions.astype(jnp.float32)[None, :] * inverse[:, None]
    return (jnp.cos(angles), jnp.sin(angles))


def rotate_rows(values, cosine_table, sine_table):
    halfway = values.shape[0] // 2
    first_half = values[:halfway]
    second_half = values[halfway:]
    return jnp.concatenate(
        [
            first_half * cosine_table - second_half * sine_table,
            second_half * cosine_table + first_half * sine_table,
        ],
        0,
    )


MESH = pl.DeviceIdType.MESH


def fused_kernel(
    ep_count,
    z_count,
    select_ref,
    q_ref,
    own_kv_ref,
    input_ref,
    gain_ref,
    gate_ref,
    up_ref,
    down_ref,
    sgate_ref,
    sup_ref,
    sdown_ref,
    chigh_ref,
    clow_ref,
    wout_ref,
    mixed_ref,
    moe_ref,
    outgoing,
    recv_a,
    buf_x,
    buf_p,
    recv_d,
    buf_s,
    recv_r,
    final,
    kv,
    heads,
    send_b,
    recv_b,
    q_t,
    m_t,
    l_t,
    acc_t,
    a_send,
    a_recv,
    k_send,
    k_recv,
    x_send,
    x_recv,
    xd_send,
    xd_recv,
    p_send,
    p_recv,
    r_send,
    r_recv,
    h_send,
    h_recv,
    hd_send,
    hd_recv,
    b_send,
    b_recv,
):
    f32, bf16 = jnp.float32, jnp.bfloat16
    ep = lax.axis_index("ep")
    tp = lax.axis_index("tp")
    z = lax.div(tp, 2)
    core = lax.rem(tp, 2)
    other = 1 - core
    half_ring = z_count // 2
    steps = half_ring - 1
    slots = ep_count * CAP
    rows = slots + MOE_DEV
    width = input_ref.shape[1]
    score_rows = NOPE + ROPE_DIM
    length = q_ref.shape[1]
    tiles = length // QTILE
    scale = float(score_rows) ** (-0.5) * LOG2E
    partner = {"tp": z * 2 + other}
    x_half = slots // 2
    r_half = rows // 2
    r_cols = width // 2
    h_half = VDIM // 2
    k_half = (score_rows + VDIM) // 2
    side_x = 4
    at_y, at_x = lax.div(ep, side_x), lax.rem(ep, side_x)

    def around(offset):
        return lax.rem(z + offset + 2 * z_count, z_count)

    def at_z(offset):
        return {"tp": around(offset) * 2 + core}

    def at_ep(offset):
        return {"ep": lax.rem(ep + offset + ep_count, ep_count)}

    def remote(src, dst, send, recv, device):
        return pltpu.make_async_remote_copy(
            src_ref=src, dst_ref=dst, send_sem=send, recv_sem=recv,
            device_id=device, device_id_type=MESH,
        )

    def loop(low, high, step):
        def run(index, carry):
            step(index)
            return carry

        lax.fori_loop(low, high, run, 0)

    def own_rows(first, count):
        return layer_scale(input_ref[pl.ds(first, count), :], gain_ref[...])

    kv[ep] = own_kv_ref[...]
    outgoing[...] = (
        lax.dot_general(
            select_ref[...],
            own_rows(tp * MOE_DEV, MOE_DEV),
            (((0,), (0,)), ((), ())),
            preferred_element_type=f32,
        )
        .reshape(ep_count, PAD, width)
        .astype(bf16)
    )

    barrier = pltpu.get_barrier_semaphore()
    loop(1, ep_count, lambda d: pl.semaphore_signal(
        barrier, inc=1, device_id=at_ep(d), device_id_type=MESH))
    for device in (at_z(1), at_z(-1), partner):
        pl.semaphore_signal(barrier, inc=1, device_id=device, device_id_type=MESH)
    pl.semaphore_wait(barrier, ep_count + 2)

    def a_copy(d):
        there = lax.rem(ep + d, ep_count)
        return remote(outgoing.at[there], recv_a.at[ep], a_send.at[d], a_recv.at[d], at_ep(d))

    def a_arrival(d):
        source = lax.rem(ep - d + ep_count, ep_count)
        return remote(outgoing.at[ep], recv_a.at[source], a_send.at[d], a_recv.at[d], at_ep(d))

    def guarded(test, act):
        @pl.when(test)
        def _():
            act()

    def k_copy(origin, half, way):
        place = (
            at_y * side_x + lax.rem(at_x + 1, side_x),
            at_y * side_x + lax.rem(at_x + side_x - 1, side_x),
            lax.rem(ep + side_x, ep_count),
            lax.rem(ep + ep_count - side_x, ep_count),
        )[way]
        part = kv.at[origin, half * k_half : (half + 1) * k_half]
        return remote(part, part, k_send.at[origin, half, way], k_recv.at[origin, half], {"ep": place})

    def k_place(origin):
        from_y, from_x = lax.div(origin, side_x), lax.rem(origin, side_x)
        return from_y, from_x, lax.rem(at_x - from_x + side_x, side_x)

    def k_pass(origin, act):
        from_y, from_x, apart = k_place(origin)
        odd = lax.rem(from_x, 2)
        same_row, same_column = at_y == from_y, apart == 0
        both, either = jnp.logical_and, jnp.logical_or
        right = either(same_column, both(apart == 1, odd == 0))
        left = either(same_column, both(apart == side_x - 1, odd == 1))
        down = either(both(same_row, at_y < side_x - 1), both(from_y == 1, at_y == 2))
        up = both(from_y == 0, either(at_y == 0, at_y == side_x - 1))
        ways = (
            (both(right, same_row), both(left, same_row), down, up),
            (right, left, both(down, same_column), both(up, same_column)),
        )
        for half in range(2):
            for way in range(4):
                guarded(ways[half][way], lambda: act(k_copy(origin, half, way)))

    def k_stage(stage):
        def take(origin):
            from_y, from_x, apart = k_place(origin)
            far = jnp.logical_or(
                jnp.logical_and(from_y == 0, at_y == 2), jnp.logical_and(from_y == 1, at_y == 3)
            )
            hops = jnp.minimum(apart, side_x - apart) + jnp.where(
                from_y == at_y, 0, jnp.where(far, 2, 1)
            )

            def act():
                for half in range(2):
                    k_copy(origin, half, 0).wait_recv()
                k_pass(origin, lambda copy: copy.start())

            guarded(jnp.logical_and(from_y <= at_y, hops == stage), act)

        loop(0, ep_count, take)

    loop(1, ep_count, lambda d: a_copy(d).start())
    k_pass(ep, lambda copy: copy.start())
    recv_a[ep] = outgoing[ep]


    def shared_rows(first, count):
        x = own_rows(first * count * 2 * MOE_DEV, count * 2 * MOE_DEV)
        hidden = jax.nn.silu(jnp.dot(x, sgate_ref[...], preferred_element_type=f32))
        hidden = (hidden * jnp.dot(x, sup_ref[...], preferred_element_type=f32)).astype(bf16)
        part = jnp.dot(hidden, sdown_ref[...], preferred_element_type=f32).astype(bf16)
        for at in range(count):
            for side in range(2):
                begin = (at * 2 + side) * MOE_DEV
                buf_p[first * count + at, side, slots:rows, :] = part[begin : begin + MOE_DEV]

    per_call = 2
    loop(0, z_count // per_call, lambda first: shared_rows(first, per_call))

    for tile in range(tiles):
        q_t[tile] = q_ref[:, tile * QTILE : (tile + 1) * QTILE]
    m_t[...] = jnp.full_like(m_t, floor_value)
    l_t[...] = jnp.zeros_like(l_t)
    acc_t[...] = jnp.zeros_like(acc_t)

    def squeeze_rows(shape, slot_dim):
        slot = lax.broadcasted_iota(jnp.int32, shape, slot_dim)
        place = lax.broadcasted_iota(jnp.int32, shape, 1 - slot_dim)
        return jnp.where(
            place == lax.div(slot, CAP) * PAD + lax.rem(slot, CAP), 1.0, 0.0
        ).astype(bf16)

    loop(1, ep_count, lambda d: a_arrival(d).wait_recv())
    arrived = recv_a[...].astype(f32).reshape(ep_count * PAD, width).astype(bf16)
    buf_x[z, core] = jnp.dot(
        squeeze_rows((slots, ep_count * PAD), 0), arrived, preferred_element_type=f32
    ).astype(bf16)

    def ring_copy(buf, send, recv, size, side, step, half, origin):
        part = pl.ds(half * size, size)
        return remote(
            buf.at[origin, core, part], buf.at[origin, core, part],
            send.at[side, step, half], recv.at[side, step, half], at_z(1 - 2 * side),
        )

    def hand_copy(buf, send, recv, size, offset, half, whose):
        part = pl.ds(half * size, size)
        here = buf.at[around(offset), whose, part]
        return remote(here, here, send.at[offset, half], recv.at[offset, half], partner)

    def x_ring(side, step, half, origin):
        return ring_copy(buf_x, x_send, x_recv, x_half, side, step, half, origin)

    def x_hand(offset, half, whose):
        return hand_copy(buf_x, xd_send, xd_recv, x_half, offset, half, whose)

    def h_ring(side, step, half, origin):
        return ring_copy(heads, h_send, h_recv, h_half, side, step, half, origin)

    def h_hand(offset, half, whose):
        return hand_copy(heads, hd_send, hd_recv, h_half, offset, half, whose)

    def offset_of(side, step):
        return step if side else z_count - step

    def begin_gather(ring, hand):
        for half in range(2):
            for side in range(2):
                ring(side, 1, half, z).start()
            hand(0, half, core).start()

    def pass_on(ring, hand, step):
        for half in range(2):
            for side in range(2):
                offset = offset_of(side, step)
                origin = around(offset)
                ring(side, step, half, origin).wait_recv()
                if half == side:
                    ring(side, step + 1, half, origin).start()
                else:
                    guarded(step < steps, lambda: ring(side, step + 1, half, origin).start())
                hand(offset, half, core).start()

    def pass_last(ring, hand):
        origin = around(half_ring)
        for side in range(2):
            ring(side, half_ring, side, origin).wait_recv()
            hand(half_ring, side, core).start()

    def take_hand(hand, offset):
        for half in range(2):
            hand(offset, half, other).wait_recv()

    def p_copy(offset):
        at = around(offset)
        return remote(buf_p.at[at, other], recv_d.at[at], p_send.at[offset], p_recv.at[offset], partner)

    def expert(offset):
        at = around(offset)
        x = buf_x[at].reshape(2 * slots, width)
        hidden = jax.nn.silu(jnp.dot(x, gate_ref[...], preferred_element_type=f32))
        hidden = (hidden * jnp.dot(x, up_ref[...], preferred_element_type=f32)).astype(bf16)
        part = jnp.dot(hidden, down_ref[...], preferred_element_type=f32).astype(bf16)
        for side in range(2):
            buf_p[at, side, 0:slots, :] = part[side * slots : (side + 1) * slots]
        p_copy(offset).start()

    def pair_sum(offset):
        at = around(offset)
        p_copy(offset).wait_recv()
        for half in range(2):
            for side in range(2):
                part = (slice(half * r_half, (half + 1) * r_half), slice(side * r_cols, (side + 1) * r_cols))
                buf_s[at, side, half] = (
                    buf_p[(at, core) + part].astype(f32) + recv_d[(at,) + part].astype(f32)
                ).astype(bf16)

    def visit(block, tile, key_count, masked):
        scores = lax.dot_general(
            block[0:score_rows, 0:key_count],
            q_t[tile],
            (((0,), (0,)), ((), ())),
            preferred_element_type=f32,
        )
        if masked:
            key_at = lax.broadcasted_iota(jnp.int32, scores.shape, 0)
            query_at = tile * QTILE + lax.broadcasted_iota(jnp.int32, scores.shape, 1)
            scores = jnp.where(key_at <= query_at, scores, floor_value)
        old_max = m_t[tile]
        new_max = jnp.maximum(old_max, jnp.max(scores, 0, keepdims=True))
        weights = jnp.exp2((scores - new_max) * scale)
        fade = jnp.exp2((old_max - new_max) * scale)
        l_t[tile] = l_t[tile] * fade + jnp.sum(weights, 0, keepdims=True)
        attended = jnp.dot(
            block[score_rows:, 0:key_count], weights.astype(bf16), preferred_element_type=f32
        )
        acc_t[tile] = acc_t[tile] * fade + attended
        m_t[tile] = new_max

    def whole_block(origin):
        for tile in range(tiles):
            visit(kv.at[origin], tile, length, False)

    def near_block(which):
        origin = ep - side_x + jnp.where(
            which == 1,
            side_x - 1,
            lax.rem(at_x + jnp.where(which == 2, 3, jnp.where(which == 3, 1, 0)), side_x) - at_x,
        )
        present = jnp.where(which == 1, at_x, at_y) > 0
        guarded(present, lambda: whole_block(origin))

    far_rows = side_x * jnp.maximum(at_y - 1, 0)
    far_count = far_rows + jnp.minimum(at_y, 1) + jnp.maximum(at_x - 1, 0)

    def part_block(unit):
        at = lax.div(unit, 2)
        which = lax.rem(unit, 2)
        row = at_y * side_x
        beside = row - side_x + lax.rem(at_x + 2, side_x)
        after = at - far_rows
        origin = jnp.where(
            after < 0,
            at,
            jnp.where(
                jnp.logical_and(after == 0, at_y > 0), beside, row + after - jnp.minimum(at_y, 1)
            ),
        )
        for tile in range(tiles // 2):
            visit(kv.at[origin], which * (tiles // 2) + tile, length, False)

    begin_gather(x_ring, x_hand)
    for tile in range(tiles):
        visit(own_kv_ref, tile, (tile + 1) * QTILE, True)
    take_hand(x_hand, 0)
    expert(0)

    def gather_step(step):
        pass_on(x_ring, x_hand, step)
        for side in range(2):
            take_hand(x_hand, offset_of(side, step))
        loop(0, 2, lambda side: expert(lax.rem(step * (2 * side - 1) + z_count, z_count)))
        k_stage(step)
        guarded(step > 1, lambda: loop(2 * step - 4, 2 * step - 2, near_block))
        loop(0, 2, lambda side: pair_sum(lax.rem(step * (2 * side - 1) + z_count, z_count)))

    loop(1, half_ring, gather_step)
    pass_last(x_ring, x_hand)

    def r_copy(step, side, half, chunk):
        return remote(
            buf_s.at[chunk, side, half], recv_r.at[step, side, half],
            r_send.at[step, side, half], r_recv.at[step, side, half], at_z(1 - 2 * side),
        )

    for half in range(2):
        for side in range(2):
            r_copy(0, side, half, around(2 * side - 1)).start()
    pair_sum(0)
    take_hand(x_hand, half_ring)
    expert(half_ring)
    pair_sum(half_ring)
    loop(half_ring, 5, k_stage)
    if half_ring < 4:
        loop(2 * half_ring - 4, 4, near_block)

    events = 4 * (z_count - 2)
    units = 2 * far_count

    def sum_event(event):
        step = lax.div(event, 4) + 1
        side = lax.rem(event, 2)
        half = lax.div(lax.rem(event, 4), 2)
        chunk = around((step + 1) * (2 * side - 1))
        r_copy(step - 1, side, half, chunk).wait_recv()
        buf_s[chunk, side, half] = (
            buf_s[chunk, side, half].astype(f32) + recv_r[step - 1, side, half].astype(f32)
        ).astype(bf16)
        r_copy(step, side, half, chunk).start()
        loop(lax.div(event * units, events), lax.div((event + 1) * units, events), part_block)

    loop(0, events, sum_event)

    for tile in range(tiles):
        heads[z, core, :, tile * QTILE : (tile + 1) * QTILE] = (acc_t[tile] / l_t[tile]).astype(bf16)
    begin_gather(h_ring, h_hand)

    for half in range(2):
        for side in range(2):
            r_copy(z_count - 2, side, half, z).wait_recv()
            final[half * r_half : (half + 1) * r_half, side * r_cols : (side + 1) * r_cols] = (
                buf_s[z, side, half].astype(f32) + recv_r[z_count - 2, side, half].astype(f32)
            )

    spread = jnp.dot(
        squeeze_rows((ep_count * PAD, slots), 1),
        final[0:slots, :].astype(bf16),
        preferred_element_type=f32,
    )
    send_b[...] = spread.reshape(ep_count, PAD, width).astype(bf16)

    def b_copy(d):
        there = lax.rem(ep + d, ep_count)
        return remote(send_b.at[there], recv_b.at[ep], b_send.at[d], b_recv.at[d], at_ep(d))

    def b_arrival(d):
        source = lax.rem(ep - d + ep_count, ep_count)
        return remote(send_b.at[ep], recv_b.at[source], b_send.at[d], b_recv.at[d], at_ep(d))

    loop(1, ep_count, lambda d: b_copy(d).start())
    recv_b[ep] = send_b[ep]

    loop(1, half_ring, lambda step: pass_on(h_ring, h_hand, step))
    pass_last(h_ring, h_hand)

    loop(1, ep_count, lambda d: b_arrival(d).wait_recv())
    returned = recv_b[...].astype(f32).reshape(ep_count * PAD, width).astype(bf16)
    moe_ref[...] = (
        jnp.dot(chigh_ref[...], returned, preferred_element_type=f32)
        + jnp.dot(clow_ref[...], returned, preferred_element_type=f32)
        + final[slots:rows, :]
    ).astype(bf16)

    loop(0, z_count, lambda offset: take_hand(h_hand, offset))
    mixed_ref[...] = lax.dot_general(
        heads[...].reshape(2 * z_count * VDIM, length),
        wout_ref[...],
        (((0,), (0,)), ((), ())),
        preferred_element_type=f32,
    ).astype(bf16)

    loop(1, ep_count, lambda d: a_copy(d).wait_send())
    loop(1, ep_count, lambda d: b_copy(d).wait_send())
    loop(
        0,
        ep_count,
        lambda origin: guarded(
            lax.div(origin, side_x) <= at_y, lambda: k_pass(origin, lambda copy: copy.wait_send())
        ),
    )

    def left(step):
        for half in range(2):
            for side in range(2):
                x_ring(side, step, half, z).wait_send()
                h_ring(side, step, half, z).wait_send()

    loop(1, half_ring, left)
    for side in range(2):
        x_ring(side, half_ring, side, z).wait_send()
        h_ring(side, half_ring, side, z).wait_send()

    def handed(offset):
        for half in range(2):
            x_hand(offset, half, core).wait_send()
            h_hand(offset, half, core).wait_send()
        p_copy(offset).wait_send()

    loop(0, z_count, handed)

    def summed(step):
        for half in range(2):
            for side in range(2):
                r_copy(step, side, half, z).wait_send()

    loop(0, z_count - 1, summed)


def fused(ep_count, tp_count, width, operands):
    f32, bf16 = jnp.float32, jnp.bfloat16
    z_count = tp_count // 2
    half_ring = z_count // 2
    slots = ep_count * CAP
    rows = slots + MOE_DEV
    score_rows, length = operands[1].shape
    tiles = length // QTILE
    dma = pltpu.SemaphoreType.DMA
    vmem = pltpu.VMEM
    return pl.pallas_call(
        functools.partial(fused_kernel, ep_count, z_count),
        out_shape=(
            jax.ShapeDtypeStruct((length, operands[-1].shape[1]), bf16),
            jax.ShapeDtypeStruct((MOE_DEV, width), bf16),
        ),
        in_specs=[pl.BlockSpec(memory_space=pltpu.VMEM)] * len(operands),
        out_specs=(pl.BlockSpec(memory_space=pltpu.VMEM),) * 2,
        scratch_shapes=[
            vmem((ep_count, PAD, width), bf16),
            vmem((ep_count, PAD, width), bf16),
            vmem((z_count, 2, slots, width), bf16),
            vmem((z_count, 2, rows, width), bf16),
            vmem((z_count, rows, width), bf16),
            vmem((z_count, 2, 2, rows // 2, width // 2), bf16),
            vmem((z_count - 1, 2, 2, rows // 2, width // 2), bf16),
            vmem((rows, width), f32),
            vmem((ep_count, score_rows + VDIM, length), bf16),
            vmem((z_count, 2, VDIM, length), bf16),
            vmem((ep_count, PAD, width), bf16),
            vmem((ep_count, PAD, width), bf16),
            vmem((tiles, score_rows, QTILE), bf16),
            vmem((tiles, 1, QTILE), f32),
            vmem((tiles, 1, QTILE), f32),
            vmem((tiles, VDIM, QTILE), f32),
            dma((ep_count,)),
            dma((ep_count,)),
            dma((ep_count, 2, 4)),
            dma((ep_count, 2)),
            dma((2, half_ring + 1, 2)),
            dma((2, half_ring + 1, 2)),
            dma((z_count, 2)),
            dma((z_count, 2)),
            dma((z_count,)),
            dma((z_count,)),
            dma((z_count - 1, 2, 2)),
            dma((z_count - 1, 2, 2)),
            dma((2, half_ring + 1, 2)),
            dma((2, half_ring + 1, 2)),
            dma((z_count, 2)),
            dma((z_count, 2)),
            dma((ep_count,)),
            dma((ep_count,)),
        ],
        compiler_params=pltpu.CompilerParams(
            collective_id=0, has_side_effects=True, vmem_limit_bytes=62 << 20
        ),
        name="fused",
    )(*operands)


def body(
    q_latent,
    kv_latent,
    rope_key,
    q_gain,
    kv_gain,
    w_query,
    w_keyval,
    w_output,
    moe_input,
    moe_gain,
    routes,
    route_weight,
    expert_gate,
    expert_up,
    expert_down,
    shared_gate,
    shared_up,
    shared_down,
):
    f32, bf16 = jnp.float32, jnp.bfloat16
    row_count = q_latent.shape[0]
    own_index = lax.axis_index("ep")
    ep_count = lax.axis_size("ep")
    tp_count = lax.axis_size("tp")
    width = moe_input.shape[1]
    top_count = routes.shape[1]

    own_block = lax.axis_index("tp")
    own_routes = lax.dynamic_slice_in_dim(routes, own_block * MOE_DEV, MOE_DEV, 0)
    own_weight = lax.dynamic_slice_in_dim(route_weight, own_block * MOE_DEV, MOE_DEV, 0)
    experts = jnp.arange(ep_count, dtype=jnp.int32)
    named = (own_routes[:, :, None] == experts).astype(f32)
    in_row = jnp.sum(named, 1)
    token_at = jnp.arange(MOE_DEV)
    before = (token_at[None, :] < token_at[:, None]).astype(f32)
    rank = jnp.dot(before, in_row, preferred_element_type=f32)
    slot_at = jnp.arange(PAD, dtype=f32)
    taken = jnp.where(
        (in_row[:, :, None] > 0) & (rank[:, :, None] == slot_at), 1.0, 0.0
    )
    weight_of = jnp.sum(named * own_weight[:, :, None], 1)
    combine = (taken * weight_of[:, :, None]).reshape(MOE_DEV, ep_count * PAD)
    select = taken.reshape(MOE_DEV, ep_count * PAD).astype(bf16)
    positions = own_index * row_count + jnp.arange(row_count, dtype=jnp.int32)
    cosine_table, sine_table = rotary_tables(positions)
    q_normed = rms_scale(q_latent, q_gain)
    kv_normed = rms_scale(kv_latent, kv_gain)
    key_rotated = rotate_rows(rope_key.T.astype(f32), cosine_table, sine_table).astype(bf16)
    projected = lax.dot_general(
        w_query, q_normed, (((0,), (1,)), ((), ())), preferred_element_type=f32
    )
    queries = jnp.concatenate(
        [projected[:NOPE], rotate_rows(projected[NOPE:], cosine_table, sine_table)], 0
    ).astype(bf16)
    expanded = lax.dot_general(
        w_keyval, kv_normed, (((0,), (1,)), ((), ())), preferred_element_type=f32
    ).astype(bf16)
    own_keyvals = jnp.concatenate([expanded[:NOPE], key_rotated, expanded[NOPE:]], 0)
    combine_high = combine.astype(bf16)
    combine_low = (combine - combine_high.astype(f32)).astype(bf16)
    mixed, moe_out = fused(
        ep_count,
        tp_count,
        width,
        (
            select,
            queries,
            own_keyvals,
            moe_input,
            moe_gain.reshape(1, width),
            expert_gate[0],
            expert_up[0],
            expert_down[0],
            shared_gate,
            shared_up,
            shared_down,
            combine_high,
            combine_low,
            w_output,
        ),
    )
    return (mixed, moe_out)


def solution(mesh):
    in_specs = (
        P("ep", None),
        P("ep", None),
        P("ep", None),
        P(),
        P(),
        P(None, "tp"),
        P(None, "tp"),
        P(None, "tp"),
        P("ep", None),
        P(),
        P("ep", None),
        P("ep", None),
        P("ep", None, "tp"),
        P("ep", None, "tp"),
        P("ep", "tp", None),
        P(None, "tp"),
        P(None, "tp"),
        P("tp", None),
    )
    out_specs = (P("ep", "tp"), P(("ep", "tp"), None))
    return jax.shard_map(body, mesh=mesh, in_specs=in_specs, out_specs=out_specs, check_vma=False)
```

```python
import functools

import jax
import jax.numpy as jnp
from jax import lax
from jax.experimental import pallas as pl
from jax.experimental.pallas import tpu as pltpu
from jax.sharding import PartitionSpec as P

NOPE = 64
ROPE_DIM = 32
VDIM = 64
MOE_DEV = 32
CAP = 6
PAD = 8

norm_eps = 1e-06
layer_eps = 1e-05
rotary_base = 10000.0
floor_value = -1e30
QTILE = 512
LOG2E = 1.4426950408889634


def rms_scale(values, gain):
    widened = values.astype(jnp.float32)
    return (
        widened * lax.rsqrt(jnp.mean(widened * widened, -1, keepdims=True) + norm_eps) * gain
    ).astype(jnp.bfloat16)


def layer_scale(values, gain):
    widened = values.astype(jnp.float32)
    centred = widened - jnp.mean(widened, -1, keepdims=True)
    return (
        centred * lax.rsqrt(jnp.mean(centred * centred, -1, keepdims=True) + layer_eps) * gain
    ).astype(jnp.bfloat16)


def rotary_tables(positions):
    halfway = ROPE_DIM // 2
    inverse = rotary_base ** (-(jnp.arange(halfway, dtype=jnp.float32) * 2.0 / ROPE_DIM))
    angles = positions.astype(jnp.float32)[None, :] * inverse[:, None]
    return (jnp.cos(angles), jnp.sin(angles))


def rotate_rows(values, cosine_table, sine_table):
    halfway = values.shape[0] // 2
    first_half = values[:halfway]
    second_half = values[halfway:]
    return jnp.concatenate(
        [
            first_half * cosine_table - second_half * sine_table,
            second_half * cosine_table + first_half * sine_table,
        ],
        0,
    )


MESH = pl.DeviceIdType.MESH
HELD = 10


def fused_kernel(
    ep_count,
    z_count,
    cosine_ref,
    sine_ref,
    rope_ref,
    q_gain_ref,
    kv_gain_ref,
    gain_ref,
    routes_ref,
    route_weight_ref,
    w_query_ref,
    w_keyval_ref,
    input_hbm,
    kv_latent_hbm,
    q_latent_hbm,
    sgate_hbm,
    sup_hbm,
    sdown_hbm,
    gate_hbm,
    up_hbm,
    down_hbm,
    wout_hbm,
    mixed_ref,
    moe_ref,
    own_ref,
    input_ref,
    kv_latent_ref,
    q_latent_ref,
    sgate_ref,
    sup_ref,
    sdown_ref,
    gate_ref,
    up_ref,
    down_ref,
    wout_ref,
    l_send,
    outgoing,
    recv_a,
    buf_x,
    buf_p,
    recv_d,
    buf_s,
    recv_r,
    final,
    kv,
    heads,
    send_b,
    recv_b,
    q_t,
    m_t,
    l_t,
    acc_t,
    a_send,
    a_recv,
    k_send,
    k_recv,
    x_send,
    x_recv,
    xd_send,
    xd_recv,
    p_send,
    p_recv,
    r_send,
    r_recv,
    h_send,
    h_recv,
    hd_send,
    hd_recv,
    b_send,
    b_recv,
):
    f32, bf16 = jnp.float32, jnp.bfloat16
    ep = lax.axis_index("ep")
    tp = lax.axis_index("tp")
    z = lax.div(tp, 2)
    core = lax.rem(tp, 2)
    other = 1 - core
    half_ring = z_count // 2
    steps = half_ring - 1
    slots = ep_count * CAP
    rows = slots + MOE_DEV
    width = input_ref.shape[1]
    score_rows = NOPE + ROPE_DIM
    length = rope_ref.shape[1]
    tiles = length // QTILE
    scale = float(score_rows) ** (-0.5) * LOG2E
    partner = {"tp": z * 2 + other}
    x_half = slots // 2
    r_half = rows // 2
    r_cols = width // 2
    h_half = VDIM // 2
    k_half = (score_rows + VDIM) // 2
    side_x = 4
    at_y, at_x = lax.div(ep, side_x), lax.rem(ep, side_x)

    def around(offset):
        return lax.rem(z + offset + 2 * z_count, z_count)

    def at_z(offset):
        return {"tp": around(offset) * 2 + core}

    def at_ep(offset):
        return {"ep": lax.rem(ep + offset + ep_count, ep_count)}

    def remote(src, dst, send, recv, device):
        return pltpu.make_async_remote_copy(
            src_ref=src, dst_ref=dst, send_sem=send, recv_sem=recv,
            device_id=device, device_id_type=MESH,
        )

    def loop(low, high, step):
        def run(index, carry):
            step(index)
            return carry

        lax.fori_loop(low, high, run, 0)

    barrier = pltpu.get_barrier_semaphore()
    loop(1, ep_count, lambda d: pl.semaphore_signal(
        barrier, inc=1, device_id=at_ep(d), device_id_type=MESH))
    for device in (at_z(1), at_z(-1), partner):
        pl.semaphore_signal(barrier, inc=1, device_id=device, device_id_type=MESH)

    first_own = pl.multiple_of(tp * MOE_DEV, MOE_DEV)
    fetches = [
        pltpu.make_async_copy(source, target, l_send.at[at])
        for at, (source, target) in enumerate(
            (
                (input_hbm.at[pl.ds(first_own, MOE_DEV)], own_ref),
                (kv_latent_hbm, kv_latent_ref),
                (q_latent_hbm, q_latent_ref),
                (input_hbm, input_ref),
                (sgate_hbm, sgate_ref),
                (sup_hbm, sup_ref),
                (sdown_hbm, sdown_ref),
                (gate_hbm, gate_ref),
                (up_hbm, up_ref),
                (down_hbm, down_ref),
                (wout_hbm, wout_ref),
            )
        )
    ]
    for fetch in fetches:
        fetch.start()

    lanes = (MOE_DEV, ep_count * PAD)
    expert_at = lax.div(lax.broadcasted_iota(jnp.int32, lanes, 1), PAD).astype(f32)
    slot_at = lax.rem(lax.broadcasted_iota(jnp.int32, lanes, 1), PAD).astype(f32)
    tokens = (MOE_DEV, routes_ref.shape[1])
    own_at = lax.broadcasted_iota(jnp.int32, tokens, 1) == (
        lax.broadcasted_iota(jnp.int32, tokens, 0) + tp * MOE_DEV
    )

    def own_column(row):
        return jnp.sum(jnp.where(own_at, row.astype(f32), 0.0), 1, keepdims=True)

    named = [
        (own_column(routes_ref[k : k + 1, :]) == expert_at).astype(f32)
        for k in range(routes_ref.shape[0])
    ]
    in_row = sum(named)
    square = (MOE_DEV, MOE_DEV)
    before = (
        lax.broadcasted_iota(jnp.int32, square, 1) < lax.broadcasted_iota(jnp.int32, square, 0)
    ).astype(bf16)
    rank = jnp.dot(before, in_row.astype(bf16), preferred_element_type=f32)
    taken = jnp.where(rank == slot_at, in_row, 0.0)
    weight_of = sum(
        named[k] * own_column(route_weight_ref[k : k + 1, :]) for k in range(len(named))
    )
    combine = taken * weight_of
    combine_high = combine.astype(bf16)
    combine_low = (combine - combine_high.astype(f32)).astype(bf16)

    fetches[0].wait()
    outgoing[...] = (
        lax.dot_general(
            taken.astype(bf16),
            layer_scale(own_ref[...], gain_ref[...]),
            (((0,), (0,)), ((), ())),
            preferred_element_type=f32,
        )
        .reshape(ep_count, PAD, width)
        .astype(bf16)
    )
    pl.semaphore_wait(barrier, ep_count + 2)

    def a_copy(d):
        there = lax.rem(ep + d, ep_count)
        return remote(outgoing.at[there], recv_a.at[ep], a_send.at[d], a_recv.at[d], at_ep(d))

    def a_arrival(d):
        source = lax.rem(ep - d + ep_count, ep_count)
        return remote(outgoing.at[ep], recv_a.at[source], a_send.at[d], a_recv.at[d], at_ep(d))

    def guarded(test, act):
        @pl.when(test)
        def _():
            act()

    def k_copy(origin, half, way):
        place = (
            at_y * side_x + lax.rem(at_x + 1, side_x),
            at_y * side_x + lax.rem(at_x + side_x - 1, side_x),
            lax.rem(ep + side_x, ep_count),
            lax.rem(ep + ep_count - side_x, ep_count),
        )[way]
        part = kv.at[origin, half * k_half : (half + 1) * k_half]
        return remote(part, part, k_send.at[origin, half, way], k_recv.at[origin, half], {"ep": place})

    def k_place(origin):
        from_y, from_x = lax.div(origin, side_x), lax.rem(origin, side_x)
        return from_y, from_x, lax.rem(at_x - from_x + side_x, side_x)

    def k_pass(origin, act):
        from_y, from_x, apart = k_place(origin)
        odd = lax.rem(from_x, 2)
        same_row, same_column = at_y == from_y, apart == 0
        both, either = jnp.logical_and, jnp.logical_or
        right = either(same_column, both(apart == 1, odd == 0))
        left = either(same_column, both(apart == side_x - 1, odd == 1))
        down = either(both(same_row, at_y < side_x - 1), both(from_y == 1, at_y == 2))
        up = both(from_y == 0, either(at_y == 0, at_y == side_x - 1))
        ways = (
            (both(right, same_row), both(left, same_row), down, up),
            (right, left, both(down, same_column), both(up, same_column)),
        )
        for half in range(2):
            for way in range(4):
                guarded(ways[half][way], lambda: act(k_copy(origin, half, way)))

    def k_stage(stage):
        def take(origin):
            from_y, from_x, apart = k_place(origin)
            far = jnp.logical_or(
                jnp.logical_and(from_y == 0, at_y == 2), jnp.logical_and(from_y == 1, at_y == 3)
            )
            hops = jnp.minimum(apart, side_x - apart) + jnp.where(
                from_y == at_y, 0, jnp.where(far, 2, 1)
            )

            def act():
                for half in range(2):
                    k_copy(origin, half, 0).wait_recv()
                k_pass(origin, lambda copy: copy.start())

            guarded(jnp.logical_and(from_y <= at_y, hops == stage), act)

        loop(0, ep_count, take)

    loop(1, ep_count, lambda d: a_copy(d).start())
    recv_a[ep] = outgoing[ep]

    transposed = (((1,), (1,)), ((), ()))
    fetches[1].wait()
    kv_normed = rms_scale(kv_latent_ref[...], kv_gain_ref[...])
    expanded = lax.dot_general(
        w_keyval_ref[...].T, kv_normed, transposed, preferred_element_type=f32
    ).astype(bf16)
    kv[ep, 0:NOPE] = expanded[0:NOPE]
    kv[ep, NOPE:score_rows] = rotate_rows(
        rope_ref[...].astype(f32), cosine_ref[...], sine_ref[...]
    ).astype(bf16)
    kv[ep, score_rows:] = expanded[NOPE:]
    fetches[2].wait()
    q_normed = rms_scale(q_latent_ref[...], q_gain_ref[...])
    projected = lax.dot_general(w_query_ref[...], q_normed, transposed, preferred_element_type=f32)
    queries = jnp.concatenate(
        [
            projected[0:NOPE],
            rotate_rows(projected[NOPE:], cosine_ref[...], sine_ref[...]),
        ],
        0,
    ).astype(bf16)
    for tile in range(tiles):
        q_t[tile] = queries[:, tile * QTILE : (tile + 1) * QTILE]


    def shared_rows(first, count):
        x = layer_scale(
            input_ref[pl.ds(first * count * 2 * MOE_DEV, count * 2 * MOE_DEV), :], gain_ref[...]
        )
        hidden = jax.nn.silu(jnp.dot(x, sgate_ref[...], preferred_element_type=f32))
        hidden = (hidden * jnp.dot(x, sup_ref[...], preferred_element_type=f32)).astype(bf16)
        part = jnp.dot(hidden, sdown_ref[...], preferred_element_type=f32).astype(bf16)
        for at in range(count):
            for side in range(2):
                begin = (at * 2 + side) * MOE_DEV
                buf_p[first * count + at, side, slots:rows, :] = part[begin : begin + MOE_DEV]

    for fetch in fetches[3:7]:
        fetch.wait()
    per_call = 2
    loop(0, z_count // per_call, lambda first: shared_rows(first, per_call))

    m_t[...] = jnp.full_like(m_t, floor_value)
    l_t[...] = jnp.zeros_like(l_t)
    acc_t[...] = jnp.zeros_like(acc_t)

    def squeeze_rows(shape, slot_dim):
        slot = lax.broadcasted_iota(jnp.int32, shape, slot_dim)
        place = lax.broadcasted_iota(jnp.int32, shape, 1 - slot_dim)
        return jnp.where(
            place == lax.div(slot, CAP) * PAD + lax.rem(slot, CAP), 1.0, 0.0
        ).astype(bf16)

    loop(1, ep_count, lambda d: a_arrival(d).wait_recv())
    arrived = recv_a[...].astype(f32).reshape(ep_count * PAD, width).astype(bf16)
    buf_x[z, core] = jnp.dot(
        squeeze_rows((slots, ep_count * PAD), 0), arrived, preferred_element_type=f32
    ).astype(bf16)

    def ring_copy(buf, send, recv, size, side, step, half, origin):
        part = pl.ds(half * size, size)
        return remote(
            buf.at[origin, core, part], buf.at[origin, core, part],
            send.at[side, step, half], recv.at[side, step, half], at_z(1 - 2 * side),
        )

    def hand_copy(buf, send, recv, size, offset, half, whose):
        part = pl.ds(half * size, size)
        here = buf.at[around(offset), whose, part]
        return remote(here, here, send.at[offset, half], recv.at[offset, half], partner)

    def x_ring(side, step, half, origin):
        return ring_copy(buf_x, x_send, x_recv, x_half, side, step, half, origin)

    def x_hand(offset, half, whose):
        return hand_copy(buf_x, xd_send, xd_recv, x_half, offset, half, whose)

    def h_ring(side, step, half, origin):
        return ring_copy(heads, h_send, h_recv, h_half, side, step, half, origin)

    def h_hand(offset, half, whose):
        return hand_copy(heads, hd_send, hd_recv, h_half, offset, half, whose)

    def offset_of(side, step):
        return step if side else z_count - step

    def begin_gather(ring, hand):
        for half in range(2):
            for side in range(2):
                ring(side, 1, half, z).start()
            hand(0, half, core).start()

    def pass_on(ring, hand, step):
        for half in range(2):
            for side in range(2):
                offset = offset_of(side, step)
                origin = around(offset)
                ring(side, step, half, origin).wait_recv()
                if half == side:
                    ring(side, step + 1, half, origin).start()
                else:
                    guarded(step < steps, lambda: ring(side, step + 1, half, origin).start())
                hand(offset, half, core).start()

    def pass_last(ring, hand):
        origin = around(half_ring)
        for side in range(2):
            ring(side, half_ring, side, origin).wait_recv()
            hand(half_ring, side, core).start()

    def take_hand(hand, offset):
        for half in range(2):
            hand(offset, half, other).wait_recv()

    def p_copy(offset):
        at = around(offset)
        return remote(buf_p.at[at, other], recv_d.at[at], p_send.at[offset], p_recv.at[offset], partner)

    def expert(offset):
        at = around(offset)
        x = buf_x[at].reshape(2 * slots, width)
        hidden = jax.nn.silu(jnp.dot(x, gate_ref[...], preferred_element_type=f32))
        hidden = (hidden * jnp.dot(x, up_ref[...], preferred_element_type=f32)).astype(bf16)
        part = jnp.dot(hidden, down_ref[...], preferred_element_type=f32).astype(bf16)
        for side in range(2):
            buf_p[at, side, 0:slots, :] = part[side * slots : (side + 1) * slots]
        p_copy(offset).start()

    def pair_sum(offset):
        at = around(offset)
        p_copy(offset).wait_recv()
        for half in range(2):
            for side in range(2):
                part = (slice(half * r_half, (half + 1) * r_half), slice(side * r_cols, (side + 1) * r_cols))
                buf_s[at, side, half] = (
                    buf_p[(at, core) + part].astype(f32) + recv_d[(at,) + part].astype(f32)
                ).astype(bf16)

    def visit(block, tile, key_count, masked):
        scores = lax.dot_general(
            block[0:score_rows, 0:key_count],
            q_t[tile],
            (((0,), (0,)), ((), ())),
            preferred_element_type=f32,
        )
        if masked:
            key_at = lax.broadcasted_iota(jnp.int32, scores.shape, 0)
            query_at = tile * QTILE + lax.broadcasted_iota(jnp.int32, scores.shape, 1)
            scores = jnp.where(key_at <= query_at, scores, floor_value)
        old_max = m_t[tile]
        new_max = jnp.maximum(old_max, jnp.max(scores, 0, keepdims=True))
        weights = jnp.exp2((scores - new_max) * scale)
        fade = jnp.exp2((old_max - new_max) * scale)
        l_t[tile] = l_t[tile] * fade + jnp.sum(weights, 0, keepdims=True)
        attended = jnp.dot(
            block[score_rows:, 0:key_count], weights.astype(bf16), preferred_element_type=f32
        )
        acc_t[tile] = acc_t[tile] * fade + attended
        m_t[tile] = new_max

    def whole_block(origin):
        for tile in range(tiles):
            visit(kv.at[origin], tile, length, False)

    def near_block(which):
        origin = ep - side_x + jnp.where(
            which == 1,
            side_x - 1,
            lax.rem(at_x + jnp.where(which == 2, 3, jnp.where(which == 3, 1, 0)), side_x) - at_x,
        )
        present = jnp.where(which == 1, at_x, at_y) > 0
        guarded(present, lambda: whole_block(origin))

    far_rows = side_x * jnp.maximum(at_y - 1, 0)
    far_count = far_rows + jnp.minimum(at_y, 1) + jnp.maximum(at_x - 1, 0)

    def part_block(unit):
        at = lax.div(unit, 2)
        which = lax.rem(unit, 2)
        row = at_y * side_x
        beside = row - side_x + lax.rem(at_x + 2, side_x)
        after = at - far_rows
        origin = jnp.where(
            after < 0,
            at,
            jnp.where(
                jnp.logical_and(after == 0, at_y > 0), beside, row + after - jnp.minimum(at_y, 1)
            ),
        )
        for tile in range(tiles // 2):
            visit(kv.at[origin], which * (tiles // 2) + tile, length, False)

    begin_gather(x_ring, x_hand)
    k_pass(ep, lambda copy: copy.start())
    for tile in range(tiles):
        visit(kv.at[ep], tile, (tile + 1) * QTILE, True)
    for fetch in fetches[7:10]:
        fetch.wait()

    def hidden_work(offset):
        take_hand(x_hand, offset)
        expert(offset)

    def beside(step, side):
        return lax.rem(step * (2 * side - 1) + z_count, z_count)

    def gather_step(step):
        pass_on(x_ring, x_hand, step)
        loop(0, jnp.minimum(step, 2), lambda side: hidden_work(beside(step - 1, side)))
        k_stage(step)
        guarded(step > 1, lambda: loop(2 * step - 4, 2 * step - 2, near_block))
        loop(0, jnp.minimum(step - 1, 2), lambda side: pair_sum(beside(step - 2, side)))

    loop(1, half_ring, gather_step)

    def r_copy(step, side, half, chunk):
        return remote(
            buf_s.at[chunk, side, half], recv_r.at[step, side, half],
            r_send.at[step, side, half], r_recv.at[step, side, half], at_z(1 - 2 * side),
        )

    def begin_sums():
        for half in range(2):
            for side in range(2):
                r_copy(0, side, half, around(2 * side - 1)).start()

    if half_ring >= 4:
        begin_sums()
    loop(0, 2, lambda side: hidden_work(beside(half_ring - 1, side)))
    pass_last(x_ring, x_hand)
    loop(half_ring, 5, k_stage)
    hidden_work(half_ring)
    loop(half_ring - 2, min(half_ring + 3, z_count), pair_sum)
    if half_ring < 4:
        begin_sums()
    if half_ring < 4:
        loop(2 * half_ring - 4, 4, near_block)

    events = 4 * (z_count - 2)
    units = 2 * far_count

    def sum_event(event):
        step = lax.div(event, 4) + 1
        side = lax.rem(event, 2)
        half = lax.div(lax.rem(event, 4), 2)
        chunk = around((step + 1) * (2 * side - 1))
        r_copy(step - 1, side, half, chunk).wait_recv()
        buf_s[chunk, side, half] = (
            buf_s[chunk, side, half].astype(f32) + recv_r[step - 1, side, half].astype(f32)
        ).astype(bf16)
        r_copy(step, side, half, chunk).start()
        loop(lax.div(event * units, events), lax.div((event + 1) * units, events), part_block)

    loop(0, events, sum_event)

    for tile in range(tiles):
        heads[z, core, :, tile * QTILE : (tile + 1) * QTILE] = (acc_t[tile] / l_t[tile]).astype(bf16)
    begin_gather(h_ring, h_hand)

    for half in range(2):
        for side in range(2):
            r_copy(z_count - 2, side, half, z).wait_recv()
            final[half * r_half : (half + 1) * r_half, side * r_cols : (side + 1) * r_cols] = (
                buf_s[z, side, half].astype(f32) + recv_r[z_count - 2, side, half].astype(f32)
            )

    spread = jnp.dot(
        squeeze_rows((ep_count * PAD, slots), 1),
        final[0:slots, :].astype(bf16),
        preferred_element_type=f32,
    )
    send_b[...] = spread.reshape(ep_count, PAD, width).astype(bf16)

    def b_copy(d):
        there = lax.rem(ep + d, ep_count)
        return remote(send_b.at[there], recv_b.at[ep], b_send.at[d], b_recv.at[d], at_ep(d))

    def b_arrival(d):
        source = lax.rem(ep - d + ep_count, ep_count)
        return remote(send_b.at[ep], recv_b.at[source], b_send.at[d], b_recv.at[d], at_ep(d))

    loop(1, ep_count, lambda d: b_copy(d).start())
    recv_b[ep] = send_b[ep]

    loop(1, half_ring, lambda step: pass_on(h_ring, h_hand, step))
    pass_last(h_ring, h_hand)

    loop(1, ep_count, lambda d: b_arrival(d).wait_recv())
    returned = recv_b[...].astype(f32).reshape(ep_count * PAD, width).astype(bf16)
    moe_ref[...] = (
        jnp.dot(combine_high, returned, preferred_element_type=f32)
        + jnp.dot(combine_low, returned, preferred_element_type=f32)
        + final[slots:rows, :]
    )

    loop(0, z_count, lambda offset: take_hand(h_hand, offset))
    fetches[10].wait()
    mixed_ref[...] = lax.dot_general(
        heads[...].reshape(2 * z_count * VDIM, length),
        wout_ref[...],
        (((0,), (0,)), ((), ())),
        preferred_element_type=f32,
    )

    loop(1, ep_count, lambda d: a_copy(d).wait_send())
    loop(1, ep_count, lambda d: b_copy(d).wait_send())
    loop(
        0,
        ep_count,
        lambda origin: guarded(
            lax.div(origin, side_x) <= at_y, lambda: k_pass(origin, lambda copy: copy.wait_send())
        ),
    )

    def left(step):
        for half in range(2):
            for side in range(2):
                x_ring(side, step, half, z).wait_send()
                h_ring(side, step, half, z).wait_send()

    loop(1, half_ring, left)
    for side in range(2):
        x_ring(side, half_ring, side, z).wait_send()
        h_ring(side, half_ring, side, z).wait_send()

    def handed(offset):
        for half in range(2):
            x_hand(offset, half, core).wait_send()
            h_hand(offset, half, core).wait_send()
        p_copy(offset).wait_send()

    loop(0, z_count, handed)

    def summed(step):
        for half in range(2):
            for side in range(2):
                r_copy(step, side, half, z).wait_send()

    loop(0, z_count - 1, summed)


def fused(ep_count, tp_count, width, operands):
    f32, bf16 = jnp.float32, jnp.bfloat16
    z_count = tp_count // 2
    half_ring = z_count // 2
    slots = ep_count * CAP
    rows = slots + MOE_DEV
    score_rows, length = NOPE + ROPE_DIM, operands[2].shape[1]
    staged = operands[HELD:]
    tiles = length // QTILE
    dma = pltpu.SemaphoreType.DMA
    vmem = pltpu.VMEM
    return pl.pallas_call(
        functools.partial(fused_kernel, ep_count, z_count),
        out_shape=(
            jax.ShapeDtypeStruct((length, operands[-1].shape[1]), f32),
            jax.ShapeDtypeStruct((MOE_DEV, width), f32),
        ),
        in_specs=[pl.BlockSpec(memory_space=pltpu.VMEM)] * HELD
        + [pl.BlockSpec(memory_space=pl.ANY)] * len(staged),
        out_specs=(pl.BlockSpec(memory_space=pltpu.VMEM),) * 2,
        scratch_shapes=[
            vmem((MOE_DEV, width), bf16),
            *[vmem(array.shape, bf16) for array in staged],
            dma((len(staged) + 1,)),
            vmem((ep_count, PAD, width), bf16),
            vmem((ep_count, PAD, width), bf16),
            vmem((z_count, 2, slots, width), bf16),
            vmem((z_count, 2, rows, width), bf16),
            vmem((z_count, rows, width), bf16),
            vmem((z_count, 2, 2, rows // 2, width // 2), bf16),
            vmem((z_count - 1, 2, 2, rows // 2, width // 2), bf16),
            vmem((rows, width), f32),
            vmem((ep_count, score_rows + VDIM, length), bf16),
            vmem((z_count, 2, VDIM, length), bf16),
            vmem((ep_count, PAD, width), bf16),
            vmem((ep_count, PAD, width), bf16),
            vmem((tiles, score_rows, QTILE), bf16),
            vmem((tiles, 1, QTILE), f32),
            vmem((tiles, 1, QTILE), f32),
            vmem((tiles, VDIM, QTILE), f32),
            dma((ep_count,)),
            dma((ep_count,)),
            dma((ep_count, 2, 4)),
            dma((ep_count, 2)),
            dma((2, half_ring + 1, 2)),
            dma((2, half_ring + 1, 2)),
            dma((z_count, 2)),
            dma((z_count, 2)),
            dma((z_count,)),
            dma((z_count,)),
            dma((z_count - 1, 2, 2)),
            dma((z_count - 1, 2, 2)),
            dma((2, half_ring + 1, 2)),
            dma((2, half_ring + 1, 2)),
            dma((z_count, 2)),
            dma((z_count, 2)),
            dma((ep_count,)),
            dma((ep_count,)),
        ],
        compiler_params=pltpu.CompilerParams(
            collective_id=0, has_side_effects=True, vmem_limit_bytes=62 << 20
        ),
        name="fused",
    )(*operands)


def body(
    q_latent,
    kv_latent,
    rope_key,
    q_gain,
    kv_gain,
    w_query,
    w_keyval,
    w_output,
    moe_input,
    moe_gain,
    routes,
    route_weight,
    expert_gate,
    expert_up,
    expert_down,
    shared_gate,
    shared_up,
    shared_down,
):
    row_count = q_latent.shape[0]
    own_index = lax.axis_index("ep")
    ep_count = lax.axis_size("ep")
    tp_count = lax.axis_size("tp")
    width = moe_input.shape[1]

    positions = own_index * row_count + jnp.arange(row_count, dtype=jnp.int32)
    cosine_table, sine_table = rotary_tables(positions)
    mixed, moe_out = fused(
        ep_count,
        tp_count,
        width,
        (
            cosine_table,
            sine_table,
            rope_key.T,
            q_gain.reshape(1, -1),
            kv_gain.reshape(1, -1),
            moe_gain.reshape(1, -1),
            routes.T,
            route_weight.T,
            w_query.T,
            w_keyval,
            moe_input,
            kv_latent,
            q_latent,
            shared_gate,
            shared_up,
            shared_down,
            expert_gate[0],
            expert_up[0],
            expert_down[0],
            w_output,
        ),
    )
    return (mixed.astype(jnp.bfloat16), moe_out.astype(jnp.bfloat16))


def solution(mesh):
    in_specs = (
        P("ep", None),
        P("ep", None),
        P("ep", None),
        P(),
        P(),
        P(None, "tp"),
        P(None, "tp"),
        P(None, "tp"),
        P("ep", None),
        P(),
        P("ep", None),
        P("ep", None),
        P("ep", None, "tp"),
        P("ep", None, "tp"),
        P("ep", "tp", None),
        P(None, "tp"),
        P(None, "tp"),
        P("tp", None),
    )
    out_specs = (P("ep", "tp"), P(("ep", "tp"), None))
    return jax.shard_map(body, mesh=mesh, in_specs=in_specs, out_specs=out_specs, check_vma=False)
```

```python
import functools

import jax
import jax.numpy as jnp
from jax import lax
from jax.experimental import pallas as pl
from jax.experimental.pallas import tpu as pltpu
from jax.sharding import PartitionSpec as P

NOPE = 64
ROPE_DIM = 32
VDIM = 64
MOE_DEV = 32
CAP = 6
PAD = 8
PACK = 3

norm_eps = 1e-06
layer_eps = 1e-05
rotary_base = 10000.0
floor_value = -1e30
QTILE = 512
LOG2E = 1.4426950408889634


def rms_scale(values, gain):
    widened = values.astype(jnp.float32)
    return (
        widened * lax.rsqrt(jnp.mean(widened * widened, -1, keepdims=True) + norm_eps) * gain
    ).astype(jnp.bfloat16)


def layer_scale(values, gain):
    widened = values.astype(jnp.float32)
    centred = widened - jnp.mean(widened, -1, keepdims=True)
    return (
        centred * lax.rsqrt(jnp.mean(centred * centred, -1, keepdims=True) + layer_eps) * gain
    ).astype(jnp.bfloat16)


def rotary_tables(positions):
    halfway = ROPE_DIM // 2
    inverse = rotary_base ** (-(jnp.arange(halfway, dtype=jnp.float32) * 2.0 / ROPE_DIM))
    angles = positions.astype(jnp.float32)[None, :] * inverse[:, None]
    return (jnp.cos(angles), jnp.sin(angles))


def rotate_rows(values, cosine_table, sine_table):
    halfway = values.shape[0] // 2
    first_half = values[:halfway]
    second_half = values[halfway:]
    return jnp.concatenate(
        [
            first_half * cosine_table - second_half * sine_table,
            second_half * cosine_table + first_half * sine_table,
        ],
        0,
    )


MESH = pl.DeviceIdType.MESH
HELD = 10


def fused_kernel(
    ep_count,
    z_count,
    cosine_ref,
    sine_ref,
    rope_ref,
    q_gain_ref,
    kv_gain_ref,
    gain_ref,
    routes_ref,
    route_weight_ref,
    w_query_ref,
    w_keyval_ref,
    input_hbm,
    kv_latent_hbm,
    q_latent_hbm,
    sgate_hbm,
    sup_hbm,
    sdown_hbm,
    gate_hbm,
    up_hbm,
    down_hbm,
    wout_hbm,
    mixed_ref,
    moe_ref,
    own_ref,
    input_ref,
    kv_latent_ref,
    q_latent_ref,
    sgate_ref,
    sup_ref,
    sdown_ref,
    gate_ref,
    up_ref,
    down_ref,
    wout_ref,
    l_send,
    outgoing,
    recv_a,
    buf_x,
    buf_p,
    recv_d,
    buf_s,
    recv_r,
    final,
    kv,
    heads,
    send_b,
    recv_b,
    q_t,
    m_t,
    l_t,
    acc_t,
    a_send,
    a_recv,
    k_send,
    k_recv,
    x_send,
    x_recv,
    xd_send,
    xd_recv,
    p_send,
    p_recv,
    r_send,
    r_recv,
    h_send,
    h_recv,
    hd_send,
    hd_recv,
    b_send,
    b_recv,
):
    f32, bf16 = jnp.float32, jnp.bfloat16
    ep = lax.axis_index("ep")
    tp = lax.axis_index("tp")
    z = lax.div(tp, 2)
    core = lax.rem(tp, 2)
    other = 1 - core
    half_ring = z_count // 2
    steps = half_ring - 1
    slots = ep_count * CAP
    rows = slots + MOE_DEV
    width = input_ref.shape[1]
    score_rows = NOPE + ROPE_DIM
    length = rope_ref.shape[1]
    tiles = length // QTILE
    scale = float(score_rows) ** (-0.5) * LOG2E
    partner = {"tp": z * 2 + other}
    x_half = slots // 2
    r_half = rows // 2
    r_cols = width // 2
    h_half = VDIM // 2
    fourth = width // 4
    k_half = (score_rows + VDIM) // 2
    side_x = 4
    at_y, at_x = lax.div(ep, side_x), lax.rem(ep, side_x)

    def columns(part):
        return slice(part * fourth, (part + 1) * fourth)

    def around(offset):
        return lax.rem(z + offset + 2 * z_count, z_count)

    def at_z(offset):
        return {"tp": around(offset) * 2 + core}

    def at_ep(offset):
        return {"ep": lax.rem(ep + offset + ep_count, ep_count)}

    def remote(src, dst, send, recv, device):
        return pltpu.make_async_remote_copy(
            src_ref=src, dst_ref=dst, send_sem=send, recv_sem=recv,
            device_id=device, device_id_type=MESH,
        )

    def loop(low, high, step):
        def run(index, carry):
            step(index)
            return carry

        lax.fori_loop(low, high, run, 0)

    barrier = pltpu.get_barrier_semaphore()
    loop(1, ep_count, lambda d: pl.semaphore_signal(
        barrier, inc=1, device_id=at_ep(d), device_id_type=MESH))
    for device in (at_z(1), at_z(-1), partner):
        pl.semaphore_signal(barrier, inc=1, device_id=device, device_id_type=MESH)

    first_own = pl.multiple_of(tp * MOE_DEV, MOE_DEV)
    fetches = [
        pltpu.make_async_copy(source, target, l_send.at[at])
        for at, (source, target) in enumerate(
            (
                (input_hbm.at[pl.ds(first_own, MOE_DEV)], own_ref),
                (kv_latent_hbm, kv_latent_ref),
                (q_latent_hbm, q_latent_ref),
                (input_hbm, input_ref),
                (sgate_hbm, sgate_ref),
                (sup_hbm, sup_ref),
                (sdown_hbm, sdown_ref),
                (gate_hbm, gate_ref),
                (up_hbm, up_ref),
                (down_hbm, down_ref),
                (wout_hbm, wout_ref),
            )
        )
    ]
    for fetch in fetches:
        fetch.start()

    lanes = (MOE_DEV, ep_count * PAD)
    expert_at = lax.div(lax.broadcasted_iota(jnp.int32, lanes, 1), PAD).astype(f32)
    slot_at = lax.rem(lax.broadcasted_iota(jnp.int32, lanes, 1), PAD).astype(f32)

    def tail_slot(part):
        low = jnp.where(slot_at == CAP, float(part), -1.0)
        return jnp.where(slot_at == CAP + 1, float(PACK + part), low)

    tokens = (MOE_DEV, routes_ref.shape[1])
    own_at = lax.broadcasted_iota(jnp.int32, tokens, 1) == (
        lax.broadcasted_iota(jnp.int32, tokens, 0) + tp * MOE_DEV
    )

    def own_column(row):
        return jnp.sum(jnp.where(own_at, row.astype(f32), 0.0), 1, keepdims=True)

    named = [
        (own_column(routes_ref[k : k + 1, :]) == expert_at).astype(f32)
        for k in range(routes_ref.shape[0])
    ]
    in_row = sum(named)
    square = (MOE_DEV, MOE_DEV)
    before = (
        lax.broadcasted_iota(jnp.int32, square, 1) < lax.broadcasted_iota(jnp.int32, square, 0)
    ).astype(bf16)
    rank = jnp.dot(before, in_row.astype(bf16), preferred_element_type=f32)
    taken = jnp.where(rank == slot_at, in_row, 0.0)
    weight_of = sum(
        named[k] * own_column(route_weight_ref[k : k + 1, :]) for k in range(len(named))
    )
    tails = [jnp.where(rank == tail_slot(part), in_row, 0.0) for part in range(PACK)]

    fetches[0].wait()
    own_normed = layer_scale(own_ref[...], gain_ref[...])

    def placed(chosen, rows_in):
        return lax.dot_general(
            chosen.astype(bf16), rows_in, (((0,), (0,)), ((), ())), preferred_element_type=f32
        )

    for part in range(PACK):
        outgoing[:, :, columns(part)] = (
            (
                placed(taken, own_normed[:, columns(part)])
                + placed(tails[part], own_normed[:, columns(PACK)])
            )
            .reshape(ep_count, PAD, fourth)
            .astype(bf16)
        )
    pl.semaphore_wait(barrier, ep_count + 2)

    def a_copy(d):
        there = lax.rem(ep + d, ep_count)
        return remote(outgoing.at[there], recv_a.at[ep], a_send.at[d], a_recv.at[d], at_ep(d))

    def a_arrival(d):
        source = lax.rem(ep - d + ep_count, ep_count)
        return remote(outgoing.at[ep], recv_a.at[source], a_send.at[d], a_recv.at[d], at_ep(d))

    def guarded(test, act):
        @pl.when(test)
        def _():
            act()

    def k_copy(origin, half, way):
        place = (
            at_y * side_x + lax.rem(at_x + 1, side_x),
            at_y * side_x + lax.rem(at_x + side_x - 1, side_x),
            lax.rem(ep + side_x, ep_count),
            lax.rem(ep + ep_count - side_x, ep_count),
        )[way]
        part = kv.at[origin, half * k_half : (half + 1) * k_half]
        return remote(part, part, k_send.at[origin, half, way], k_recv.at[origin, half], {"ep": place})

    def k_place(origin):
        from_y, from_x = lax.div(origin, side_x), lax.rem(origin, side_x)
        return from_y, from_x, lax.rem(at_x - from_x + side_x, side_x)

    def k_pass(origin, act):
        from_y, from_x, apart = k_place(origin)
        odd = lax.rem(from_x, 2)
        same_row, same_column = at_y == from_y, apart == 0
        both, either = jnp.logical_and, jnp.logical_or
        right = either(same_column, both(apart == 1, odd == 0))
        left = either(same_column, both(apart == side_x - 1, odd == 1))
        down = either(both(same_row, at_y < side_x - 1), both(from_y == 1, at_y == 2))
        up = both(from_y == 0, either(at_y == 0, at_y == side_x - 1))
        ways = (
            (both(right, same_row), both(left, same_row), down, up),
            (right, left, both(down, same_column), both(up, same_column)),
        )
        for half in range(2):
            for way in range(4):
                guarded(ways[half][way], lambda: act(k_copy(origin, half, way)))

    def k_stage(stage):
        def take(origin):
            from_y, from_x, apart = k_place(origin)
            far = jnp.logical_or(
                jnp.logical_and(from_y == 0, at_y == 2), jnp.logical_and(from_y == 1, at_y == 3)
            )
            hops = jnp.minimum(apart, side_x - apart) + jnp.where(
                from_y == at_y, 0, jnp.where(far, 2, 1)
            )

            def act():
                for half in range(2):
                    k_copy(origin, half, 0).wait_recv()
                k_pass(origin, lambda copy: copy.start())

            guarded(jnp.logical_and(from_y <= at_y, hops == stage), act)

        loop(0, ep_count, take)

    loop(1, ep_count, lambda d: a_copy(d).start())
    recv_a[ep] = outgoing[ep]

    transposed = (((1,), (1,)), ((), ()))
    fetches[1].wait()
    kv_normed = rms_scale(kv_latent_ref[...], kv_gain_ref[...])
    expanded = lax.dot_general(
        w_keyval_ref[...].T, kv_normed, transposed, preferred_element_type=f32
    ).astype(bf16)
    kv[ep, 0:NOPE] = expanded[0:NOPE]
    kv[ep, NOPE:score_rows] = rotate_rows(
        rope_ref[...].astype(f32), cosine_ref[...], sine_ref[...]
    ).astype(bf16)
    kv[ep, score_rows:] = expanded[NOPE:]
    fetches[2].wait()
    q_normed = rms_scale(q_latent_ref[...], q_gain_ref[...])
    projected = lax.dot_general(w_query_ref[...], q_normed, transposed, preferred_element_type=f32)
    queries = jnp.concatenate(
        [
            projected[0:NOPE],
            rotate_rows(projected[NOPE:], cosine_ref[...], sine_ref[...]),
        ],
        0,
    ).astype(bf16)
    for tile in range(tiles):
        q_t[tile] = queries[:, tile * QTILE : (tile + 1) * QTILE]


    def shared_rows(first, count):
        x = layer_scale(
            input_ref[pl.ds(first * count * 2 * MOE_DEV, count * 2 * MOE_DEV), :], gain_ref[...]
        )
        hidden = jax.nn.silu(jnp.dot(x, sgate_ref[...], preferred_element_type=f32))
        hidden = (hidden * jnp.dot(x, sup_ref[...], preferred_element_type=f32)).astype(bf16)
        part = jnp.dot(hidden, sdown_ref[...], preferred_element_type=f32).astype(bf16)
        for at in range(count):
            for side in range(2):
                begin = (at * 2 + side) * MOE_DEV
                buf_p[first * count + at, side, slots:rows, :] = part[begin : begin + MOE_DEV]

    for fetch in fetches[3:7]:
        fetch.wait()
    per_call = 2
    loop(0, z_count // per_call, lambda first: shared_rows(first, per_call))

    m_t[...] = jnp.full_like(m_t, floor_value)
    l_t[...] = jnp.zeros_like(l_t)
    acc_t[...] = jnp.zeros_like(acc_t)

    def squeeze_rows(shape, slot_dim, part=None):
        slot = lax.broadcasted_iota(jnp.int32, shape, slot_dim)
        place = lax.broadcasted_iota(jnp.int32, shape, 1 - slot_dim)
        expert, number = lax.div(slot, CAP), lax.rem(slot, CAP)
        if part is None:
            return jnp.where(place == expert * PAD + number, 1.0, 0.0).astype(bf16)
        target = expert * PAD + CAP + lax.div(number, PACK)
        here = jnp.logical_and(place == target, lax.rem(number, PACK) == part)
        return jnp.where(here, 1.0, 0.0).astype(bf16)

    loop(1, ep_count, lambda d: a_arrival(d).wait_recv())
    arrived = recv_a[...].astype(f32).reshape(ep_count * PAD, PACK * fourth).astype(bf16)
    packed_shape = (slots, ep_count * PAD)
    last = 0.0
    for part in range(PACK):
        piece = arrived[:, columns(part)]
        buf_x[z, core, :, columns(part)] = jnp.dot(
            squeeze_rows(packed_shape, 0), piece, preferred_element_type=f32
        ).astype(bf16)
        last += jnp.dot(squeeze_rows(packed_shape, 0, part), piece, preferred_element_type=f32)
    buf_x[z, core, :, columns(PACK)] = last.astype(bf16)

    def ring_copy(buf, send, recv, size, side, step, half, origin):
        part = pl.ds(half * size, size)
        return remote(
            buf.at[origin, core, part], buf.at[origin, core, part],
            send.at[side, step, half], recv.at[side, step, half], at_z(1 - 2 * side),
        )

    def hand_copy(buf, send, recv, size, offset, half, whose):
        part = pl.ds(half * size, size)
        here = buf.at[around(offset), whose, part]
        return remote(here, here, send.at[offset, half], recv.at[offset, half], partner)

    def x_ring(side, step, half, origin):
        return ring_copy(buf_x, x_send, x_recv, x_half, side, step, half, origin)

    def x_hand(offset, half, whose):
        return hand_copy(buf_x, xd_send, xd_recv, x_half, offset, half, whose)

    def h_ring(side, step, half, origin):
        return ring_copy(heads, h_send, h_recv, h_half, side, step, half, origin)

    def h_hand(offset, half, whose):
        return hand_copy(heads, hd_send, hd_recv, h_half, offset, half, whose)

    def offset_of(side, step):
        return step if side else z_count - step

    def begin_gather(ring, hand):
        for half in range(2):
            for side in range(2):
                ring(side, 1, half, z).start()
            hand(0, half, core).start()

    def pass_on(ring, hand, step):
        for half in range(2):
            for side in range(2):
                offset = offset_of(side, step)
                origin = around(offset)
                ring(side, step, half, origin).wait_recv()
                if half == side:
                    ring(side, step + 1, half, origin).start()
                else:
                    guarded(step < steps, lambda: ring(side, step + 1, half, origin).start())
                hand(offset, half, core).start()

    def pass_last(ring, hand):
        origin = around(half_ring)
        for side in range(2):
            ring(side, half_ring, side, origin).wait_recv()
            hand(half_ring, side, core).start()

    def take_hand(hand, offset):
        for half in range(2):
            hand(offset, half, other).wait_recv()

    def p_copy(offset):
        at = around(offset)
        return remote(buf_p.at[at, other], recv_d.at[at], p_send.at[offset], p_recv.at[offset], partner)

    def expert(offset):
        at = around(offset)
        x = buf_x[at].reshape(2 * slots, width)
        hidden = jax.nn.silu(jnp.dot(x, gate_ref[...], preferred_element_type=f32))
        hidden = (hidden * jnp.dot(x, up_ref[...], preferred_element_type=f32)).astype(bf16)
        part = jnp.dot(hidden, down_ref[...], preferred_element_type=f32).astype(bf16)
        for side in range(2):
            buf_p[at, side, 0:slots, :] = part[side * slots : (side + 1) * slots]
        p_copy(offset).start()

    def pair_sum(offset):
        at = around(offset)
        p_copy(offset).wait_recv()
        for half in range(2):
            for side in range(2):
                part = (slice(half * r_half, (half + 1) * r_half), slice(side * r_cols, (side + 1) * r_cols))
                buf_s[at, side, half] = (
                    buf_p[(at, core) + part].astype(f32) + recv_d[(at,) + part].astype(f32)
                ).astype(bf16)

    def visit(block, tile, key_count, masked):
        scores = lax.dot_general(
            block[0:score_rows, 0:key_count],
            q_t[tile],
            (((0,), (0,)), ((), ())),
            preferred_element_type=f32,
        )
        if masked:
            key_at = lax.broadcasted_iota(jnp.int32, scores.shape, 0)
            query_at = tile * QTILE + lax.broadcasted_iota(jnp.int32, scores.shape, 1)
            scores = jnp.where(key_at <= query_at, scores, floor_value)
        old_max = m_t[tile]
        new_max = jnp.maximum(old_max, jnp.max(scores, 0, keepdims=True))
        weights = jnp.exp2((scores - new_max) * scale)
        fade = jnp.exp2((old_max - new_max) * scale)
        l_t[tile] = l_t[tile] * fade + jnp.sum(weights, 0, keepdims=True)
        attended = jnp.dot(
            block[score_rows:, 0:key_count], weights.astype(bf16), preferred_element_type=f32
        )
        acc_t[tile] = acc_t[tile] * fade + attended
        m_t[tile] = new_max

    def whole_block(origin):
        for tile in range(tiles):
            visit(kv.at[origin], tile, length, False)

    def near_block(which):
        origin = ep - side_x + jnp.where(
            which == 1,
            side_x - 1,
            lax.rem(at_x + jnp.where(which == 2, 3, jnp.where(which == 3, 1, 0)), side_x) - at_x,
        )
        present = jnp.where(which == 1, at_x, at_y) > 0
        guarded(present, lambda: whole_block(origin))

    far_rows = side_x * jnp.maximum(at_y - 1, 0)
    far_count = far_rows + jnp.minimum(at_y, 1) + jnp.maximum(at_x - 1, 0)

    def part_block(unit):
        at = lax.div(unit, 2)
        which = lax.rem(unit, 2)
        row = at_y * side_x
        beside = row - side_x + lax.rem(at_x + 2, side_x)
        after = at - far_rows
        origin = jnp.where(
            after < 0,
            at,
            jnp.where(
                jnp.logical_and(after == 0, at_y > 0), beside, row + after - jnp.minimum(at_y, 1)
            ),
        )
        for tile in range(tiles // 2):
            visit(kv.at[origin], which * (tiles // 2) + tile, length, False)

    begin_gather(x_ring, x_hand)
    k_pass(ep, lambda copy: copy.start())
    for tile in range(tiles):
        visit(kv.at[ep], tile, (tile + 1) * QTILE, True)
    for fetch in fetches[7:10]:
        fetch.wait()

    def hidden_work(offset):
        take_hand(x_hand, offset)
        expert(offset)

    def beside(step, side):
        return lax.rem(step * (2 * side - 1) + z_count, z_count)

    def gather_step(step):
        pass_on(x_ring, x_hand, step)
        loop(0, jnp.minimum(step, 2), lambda side: hidden_work(beside(step - 1, side)))
        guarded(step < 3, lambda: k_stage(step))
        guarded(step > 1, lambda: loop(2 * step - 4, 2 * step - 2, near_block))
        loop(0, jnp.minimum(step - 1, 2), lambda side: pair_sum(beside(step - 2, side)))

    loop(1, half_ring, gather_step)

    def r_copy(step, side, half, chunk):
        return remote(
            buf_s.at[chunk, side, half], recv_r.at[step, side, half],
            r_send.at[step, side, half], r_recv.at[step, side, half], at_z(1 - 2 * side),
        )

    def begin_sums():
        for half in range(2):
            for side in range(2):
                r_copy(0, side, half, around(2 * side - 1)).start()

    if half_ring >= 4:
        begin_sums()
    loop(0, 2, lambda side: hidden_work(beside(half_ring - 1, side)))
    pass_last(x_ring, x_hand)
    if half_ring >= 4:
        k_stage(3)
    else:
        loop(half_ring, 4, k_stage)
    hidden_work(half_ring)
    loop(half_ring - 2, min(half_ring + 3, z_count), pair_sum)
    if half_ring < 4:
        begin_sums()
    if half_ring < 4:
        loop(2 * half_ring - 4, 4, near_block)

    events = 4 * (z_count - 2)
    units = 2 * far_count
    quiet = 4

    def sum_event(event):
        step = lax.div(event, 4) + 1
        side = lax.rem(event, 2)
        half = lax.div(lax.rem(event, 4), 2)
        chunk = around((step + 1) * (2 * side - 1))
        r_copy(step - 1, side, half, chunk).wait_recv()
        buf_s[chunk, side, half] = (
            buf_s[chunk, side, half].astype(f32) + recv_r[step - 1, side, half].astype(f32)
        ).astype(bf16)
        r_copy(step, side, half, chunk).start()
        guarded(event == quiet - 1, lambda: k_stage(4))
        done = jnp.maximum(event - quiet, 0) * units
        due = jnp.maximum(event + 1 - quiet, 0) * units
        loop(lax.div(done, events - quiet), lax.div(due, events - quiet), part_block)

    loop(0, events, sum_event)

    for tile in range(tiles):
        heads[z, core, :, tile * QTILE : (tile + 1) * QTILE] = (acc_t[tile] / l_t[tile]).astype(bf16)
    begin_gather(h_ring, h_hand)

    for half in range(2):
        for side in range(2):
            r_copy(z_count - 2, side, half, z).wait_recv()
            final[half * r_half : (half + 1) * r_half, side * r_cols : (side + 1) * r_cols] = (
                buf_s[z, side, half].astype(f32) + recv_r[z_count - 2, side, half].astype(f32)
            )

    sums = final[0:slots, :].astype(bf16)
    spread_shape = (ep_count * PAD, slots)
    for part in range(PACK):
        spread = jnp.dot(
            squeeze_rows(spread_shape, 1), sums[:, columns(part)], preferred_element_type=f32
        ) + jnp.dot(
            squeeze_rows(spread_shape, 1, part), sums[:, columns(PACK)], preferred_element_type=f32
        )
        send_b[:, :, columns(part)] = spread.reshape(ep_count, PAD, fourth).astype(bf16)

    def b_copy(d):
        there = lax.rem(ep + d, ep_count)
        return remote(send_b.at[there], recv_b.at[ep], b_send.at[d], b_recv.at[d], at_ep(d))

    def b_arrival(d):
        source = lax.rem(ep - d + ep_count, ep_count)
        return remote(send_b.at[ep], recv_b.at[source], b_send.at[d], b_recv.at[d], at_ep(d))

    loop(1, ep_count, lambda d: b_copy(d).start())
    recv_b[ep] = send_b[ep]

    loop(1, half_ring, lambda step: pass_on(h_ring, h_hand, step))
    pass_last(h_ring, h_hand)

    loop(1, ep_count, lambda d: b_arrival(d).wait_recv())
    returned = recv_b[...].astype(f32).reshape(ep_count * PAD, PACK * fourth).astype(bf16)

    def weighed(chosen, rows_in):
        combine = chosen * weight_of
        high = combine.astype(bf16)
        low = (combine - high.astype(f32)).astype(bf16)
        return jnp.dot(high, rows_in, preferred_element_type=f32) + jnp.dot(
            low, rows_in, preferred_element_type=f32
        )

    last = final[slots:rows, columns(PACK)]
    for part in range(PACK):
        piece = returned[:, columns(part)]
        moe_ref[:, columns(part)] = weighed(taken, piece) + final[slots:rows, columns(part)]
        last += weighed(tails[part], piece)
    moe_ref[:, columns(PACK)] = last

    loop(0, z_count, lambda offset: take_hand(h_hand, offset))
    fetches[10].wait()
    mixed_ref[...] = lax.dot_general(
        heads[...].reshape(2 * z_count * VDIM, length),
        wout_ref[...],
        (((0,), (0,)), ((), ())),
        preferred_element_type=f32,
    )

    loop(1, ep_count, lambda d: a_copy(d).wait_send())
    loop(1, ep_count, lambda d: b_copy(d).wait_send())
    loop(
        0,
        ep_count,
        lambda origin: guarded(
            lax.div(origin, side_x) <= at_y, lambda: k_pass(origin, lambda copy: copy.wait_send())
        ),
    )

    def left(step):
        for half in range(2):
            for side in range(2):
                x_ring(side, step, half, z).wait_send()
                h_ring(side, step, half, z).wait_send()

    loop(1, half_ring, left)
    for side in range(2):
        x_ring(side, half_ring, side, z).wait_send()
        h_ring(side, half_ring, side, z).wait_send()

    def handed(offset):
        for half in range(2):
            x_hand(offset, half, core).wait_send()
            h_hand(offset, half, core).wait_send()
        p_copy(offset).wait_send()

    loop(0, z_count, handed)

    def summed(step):
        for half in range(2):
            for side in range(2):
                r_copy(step, side, half, z).wait_send()

    loop(0, z_count - 1, summed)


def fused(ep_count, tp_count, width, operands):
    f32, bf16 = jnp.float32, jnp.bfloat16
    z_count = tp_count // 2
    half_ring = z_count // 2
    slots = ep_count * CAP
    rows = slots + MOE_DEV
    score_rows, length = NOPE + ROPE_DIM, operands[2].shape[1]
    staged = operands[HELD:]
    tiles = length // QTILE
    dma = pltpu.SemaphoreType.DMA
    vmem = pltpu.VMEM
    return pl.pallas_call(
        functools.partial(fused_kernel, ep_count, z_count),
        out_shape=(
            jax.ShapeDtypeStruct((length, operands[-1].shape[1]), f32),
            jax.ShapeDtypeStruct((MOE_DEV, width), f32),
        ),
        in_specs=[pl.BlockSpec(memory_space=pltpu.VMEM)] * HELD
        + [pl.BlockSpec(memory_space=pl.ANY)] * len(staged),
        out_specs=(pl.BlockSpec(memory_space=pltpu.VMEM),) * 2,
        scratch_shapes=[
            vmem((MOE_DEV, width), bf16),
            *[vmem(array.shape, bf16) for array in staged],
            dma((len(staged) + 1,)),
            vmem((ep_count, PAD, width // 4 * PACK), bf16),
            vmem((ep_count, PAD, width // 4 * PACK), bf16),
            vmem((z_count, 2, slots, width), bf16),
            vmem((z_count, 2, rows, width), bf16),
            vmem((z_count, rows, width), bf16),
            vmem((z_count, 2, 2, rows // 2, width // 2), bf16),
            vmem((z_count - 1, 2, 2, rows // 2, width // 2), bf16),
            vmem((rows, width), f32),
            vmem((ep_count, score_rows + VDIM, length), bf16),
            vmem((z_count, 2, VDIM, length), bf16),
            vmem((ep_count, PAD, width // 4 * PACK), bf16),
            vmem((ep_count, PAD, width // 4 * PACK), bf16),
            vmem((tiles, score_rows, QTILE), bf16),
            vmem((tiles, 1, QTILE), f32),
            vmem((tiles, 1, QTILE), f32),
            vmem((tiles, VDIM, QTILE), f32),
            dma((ep_count,)),
            dma((ep_count,)),
            dma((ep_count, 2, 4)),
            dma((ep_count, 2)),
            dma((2, half_ring + 1, 2)),
            dma((2, half_ring + 1, 2)),
            dma((z_count, 2)),
            dma((z_count, 2)),
            dma((z_count,)),
            dma((z_count,)),
            dma((z_count - 1, 2, 2)),
            dma((z_count - 1, 2, 2)),
            dma((2, half_ring + 1, 2)),
            dma((2, half_ring + 1, 2)),
            dma((z_count, 2)),
            dma((z_count, 2)),
            dma((ep_count,)),
            dma((ep_count,)),
        ],
        compiler_params=pltpu.CompilerParams(
            collective_id=0, has_side_effects=True, vmem_limit_bytes=62 << 20
        ),
        name="fused",
    )(*operands)


def body(
    q_latent,
    kv_latent,
    rope_key,
    q_gain,
    kv_gain,
    w_query,
    w_keyval,
    w_output,
    moe_input,
    moe_gain,
    routes,
    route_weight,
    expert_gate,
    expert_up,
    expert_down,
    shared_gate,
    shared_up,
    shared_down,
):
    row_count = q_latent.shape[0]
    own_index = lax.axis_index("ep")
    ep_count = lax.axis_size("ep")
    tp_count = lax.axis_size("tp")
    width = moe_input.shape[1]

    positions = own_index * row_count + jnp.arange(row_count, dtype=jnp.int32)
    cosine_table, sine_table = rotary_tables(positions)
    mixed, moe_out = fused(
        ep_count,
        tp_count,
        width,
        (
            cosine_table,
            sine_table,
            rope_key.T,
            q_gain.reshape(1, -1),
            kv_gain.reshape(1, -1),
            moe_gain.reshape(1, -1),
            routes.T,
            route_weight.T,
            w_query.T,
            w_keyval,
            moe_input,
            kv_latent,
            q_latent,
            shared_gate,
            shared_up,
            shared_down,
            expert_gate[0],
            expert_up[0],
            expert_down[0],
            w_output,
        ),
    )
    return (mixed.astype(jnp.bfloat16), moe_out.astype(jnp.bfloat16))


def solution(mesh):
    in_specs = (
        P("ep", None),
        P("ep", None),
        P("ep", None),
        P(),
        P(),
        P(None, "tp"),
        P(None, "tp"),
        P(None, "tp"),
        P("ep", None),
        P(),
        P("ep", None),
        P("ep", None),
        P("ep", None, "tp"),
        P("ep", None, "tp"),
        P("ep", "tp", None),
        P(None, "tp"),
        P(None, "tp"),
        P("tp", None),
    )
    out_specs = (P("ep", "tp"), P(("ep", "tp"), None))
    return jax.shard_map(body, mesh=mesh, in_specs=in_specs, out_specs=out_specs, check_vma=False)
```

```python
import functools

import jax
import jax.numpy as jnp
from jax import lax
from jax.experimental import pallas as pl
from jax.experimental.pallas import tpu as pltpu
from jax.sharding import PartitionSpec as P

NOPE = 64
ROPE_DIM = 32
VDIM = 64
MOE_DEV = 32
CAP = 6
PAD = 8
PACK = 3

norm_eps = 1e-06
layer_eps = 1e-05
rotary_base = 10000.0
floor_value = -1e30
QTILE = 512
LOG2E = 1.4426950408889634


def rms_scale(values, gain):
    widened = values.astype(jnp.float32)
    return (
        widened * lax.rsqrt(jnp.mean(widened * widened, -1, keepdims=True) + norm_eps) * gain
    ).astype(jnp.bfloat16)


def layer_scale(values, gain):
    widened = values.astype(jnp.float32)
    centred = widened - jnp.mean(widened, -1, keepdims=True)
    return (
        centred * lax.rsqrt(jnp.mean(centred * centred, -1, keepdims=True) + layer_eps) * gain
    ).astype(jnp.bfloat16)


def rotary_tables(positions):
    halfway = ROPE_DIM // 2
    inverse = rotary_base ** (-(jnp.arange(halfway, dtype=jnp.float32) * 2.0 / ROPE_DIM))
    angles = positions.astype(jnp.float32)[None, :] * inverse[:, None]
    return (jnp.cos(angles), jnp.sin(angles))


def rotate_rows(values, cosine_table, sine_table):
    halfway = values.shape[0] // 2
    first_half = values[:halfway]
    second_half = values[halfway:]
    return jnp.concatenate(
        [
            first_half * cosine_table - second_half * sine_table,
            second_half * cosine_table + first_half * sine_table,
        ],
        0,
    )


MESH = pl.DeviceIdType.MESH
HELD = 10


def fused_kernel(
    ep_count,
    z_count,
    cosine_ref,
    sine_ref,
    rope_ref,
    q_gain_ref,
    kv_gain_ref,
    gain_ref,
    routes_ref,
    route_weight_ref,
    w_query_ref,
    w_keyval_ref,
    input_hbm,
    kv_latent_hbm,
    q_latent_hbm,
    sgate_hbm,
    sup_hbm,
    sdown_hbm,
    gate_hbm,
    up_hbm,
    down_hbm,
    wout_hbm,
    mixed_ref,
    moe_ref,
    own_ref,
    input_ref,
    kv_latent_ref,
    q_latent_ref,
    sgate_ref,
    sup_ref,
    sdown_ref,
    gate_ref,
    up_ref,
    down_ref,
    wout_ref,
    l_send,
    outgoing,
    recv_a,
    buf_x,
    buf_p,
    recv_d,
    buf_s,
    recv_r,
    final,
    kv,
    heads,
    send_b,
    recv_b,
    q_t,
    m_t,
    l_t,
    acc_t,
    a_send,
    a_recv,
    k_send,
    k_recv,
    x_send,
    x_recv,
    xd_send,
    xd_recv,
    p_send,
    p_recv,
    r_send,
    r_recv,
    h_send,
    h_recv,
    hd_send,
    hd_recv,
    b_send,
    b_recv,
):
    f32, bf16 = jnp.float32, jnp.bfloat16
    ep = lax.axis_index("ep")
    tp = lax.axis_index("tp")
    z = lax.div(tp, 2)
    core = lax.rem(tp, 2)
    other = 1 - core
    half_ring = z_count // 2
    steps = half_ring - 1
    slots = ep_count * CAP
    rows = slots + MOE_DEV
    width = input_ref.shape[1]
    score_rows = NOPE + ROPE_DIM
    length = rope_ref.shape[1]
    tiles = length // QTILE
    scale = float(score_rows) ** (-0.5) * LOG2E
    partner = {"tp": z * 2 + other}
    x_half = slots // 2
    r_half = rows // 2
    r_cols = width // 2
    h_half = VDIM // 2
    fourth = width // 4
    k_half = (score_rows + VDIM) // 2
    side_x = 4
    at_y, at_x = lax.div(ep, side_x), lax.rem(ep, side_x)

    def columns(part):
        return slice(part * fourth, (part + 1) * fourth)

    def around(offset):
        return lax.rem(z + offset + 2 * z_count, z_count)

    def at_z(offset):
        return {"tp": around(offset) * 2 + core}

    def at_ep(offset):
        return {"ep": lax.rem(ep + offset + ep_count, ep_count)}

    def remote(src, dst, send, recv, device):
        return pltpu.make_async_remote_copy(
            src_ref=src, dst_ref=dst, send_sem=send, recv_sem=recv,
            device_id=device, device_id_type=MESH,
        )

    def loop(low, high, step):
        def run(index, carry):
            step(index)
            return carry

        lax.fori_loop(low, high, run, 0)

    barrier = pltpu.get_barrier_semaphore()
    loop(1, ep_count, lambda d: pl.semaphore_signal(
        barrier, inc=1, device_id=at_ep(d), device_id_type=MESH))
    for device in (at_z(1), at_z(-1), partner):
        pl.semaphore_signal(barrier, inc=1, device_id=device, device_id_type=MESH)

    first_own = pl.multiple_of(tp * MOE_DEV, MOE_DEV)
    fetches = [
        pltpu.make_async_copy(source, target, l_send.at[at])
        for at, (source, target) in enumerate(
            (
                (input_hbm.at[pl.ds(first_own, MOE_DEV)], own_ref),
                (kv_latent_hbm, kv_latent_ref),
                (q_latent_hbm, q_latent_ref),
                (input_hbm, input_ref),
                (sgate_hbm, sgate_ref),
                (sup_hbm, sup_ref),
                (sdown_hbm, sdown_ref),
                (gate_hbm, gate_ref),
                (up_hbm, up_ref),
                (down_hbm, down_ref),
                (wout_hbm, wout_ref),
            )
        )
    ]
    for fetch in fetches:
        fetch.start()

    lanes = (MOE_DEV, ep_count * PAD)
    expert_at = lax.div(lax.broadcasted_iota(jnp.int32, lanes, 1), PAD).astype(f32)
    slot_at = lax.rem(lax.broadcasted_iota(jnp.int32, lanes, 1), PAD).astype(f32)

    def tail_slot(part):
        low = jnp.where(slot_at == CAP, float(part), -1.0)
        return jnp.where(slot_at == CAP + 1, float(PACK + part), low)

    tokens = (MOE_DEV, routes_ref.shape[1])
    own_at = lax.broadcasted_iota(jnp.int32, tokens, 1) == (
        lax.broadcasted_iota(jnp.int32, tokens, 0) + tp * MOE_DEV
    )

    def own_column(row):
        return jnp.sum(jnp.where(own_at, row.astype(f32), 0.0), 1, keepdims=True)

    named = [
        (own_column(routes_ref[k : k + 1, :]) == expert_at).astype(f32)
        for k in range(routes_ref.shape[0])
    ]
    in_row = sum(named)
    square = (MOE_DEV, MOE_DEV)
    before = (
        lax.broadcasted_iota(jnp.int32, square, 1) < lax.broadcasted_iota(jnp.int32, square, 0)
    ).astype(bf16)
    rank = jnp.dot(before, in_row.astype(bf16), preferred_element_type=f32)
    taken = jnp.where(rank == slot_at, in_row, 0.0)
    weight_of = sum(
        named[k] * own_column(route_weight_ref[k : k + 1, :]) for k in range(len(named))
    )
    tails = [jnp.where(rank == tail_slot(part), in_row, 0.0) for part in range(PACK)]

    fetches[0].wait()
    own_normed = layer_scale(own_ref[...], gain_ref[...])

    def placed(chosen, rows_in):
        return lax.dot_general(
            chosen.astype(bf16), rows_in, (((0,), (0,)), ((), ())), preferred_element_type=f32
        )

    for part in range(PACK):
        outgoing[:, :, columns(part)] = (
            (
                placed(taken, own_normed[:, columns(part)])
                + placed(tails[part], own_normed[:, columns(PACK)])
            )
            .reshape(ep_count, PAD, fourth)
            .astype(bf16)
        )
    pl.semaphore_wait(barrier, ep_count + 2)

    def a_copy(d):
        there = lax.rem(ep + d, ep_count)
        return remote(outgoing.at[there], recv_a.at[ep], a_send.at[d], a_recv.at[d], at_ep(d))

    def a_arrival(d):
        source = lax.rem(ep - d + ep_count, ep_count)
        return remote(outgoing.at[ep], recv_a.at[source], a_send.at[d], a_recv.at[d], at_ep(d))

    def guarded(test, act):
        @pl.when(test)
        def _():
            act()

    def k_copy(origin, half, way):
        place = (
            at_y * side_x + lax.rem(at_x + 1, side_x),
            at_y * side_x + lax.rem(at_x + side_x - 1, side_x),
            lax.rem(ep + side_x, ep_count),
            lax.rem(ep + ep_count - side_x, ep_count),
        )[way]
        part = kv.at[origin, half * k_half : (half + 1) * k_half]
        return remote(part, part, k_send.at[origin, half, way], k_recv.at[origin, half], {"ep": place})

    def k_place(origin):
        from_y, from_x = lax.div(origin, side_x), lax.rem(origin, side_x)
        return from_y, from_x, lax.rem(at_x - from_x + side_x, side_x)

    def k_pass(origin, act):
        from_y, from_x, apart = k_place(origin)
        odd = lax.rem(from_x, 2)
        same_row, same_column = at_y == from_y, apart == 0
        both, either = jnp.logical_and, jnp.logical_or
        right = either(same_column, both(apart == 1, odd == 0))
        left = either(same_column, both(apart == side_x - 1, odd == 1))
        down = either(both(same_row, at_y < side_x - 1), both(from_y == 1, at_y == 2))
        up = both(from_y == 0, either(at_y == 0, at_y == side_x - 1))
        ways = (
            (both(right, same_row), both(left, same_row), down, up),
            (right, left, both(down, same_column), both(up, same_column)),
        )
        for half in range(2):
            for way in range(4):
                guarded(ways[half][way], lambda: act(k_copy(origin, half, way)))

    def k_stage(stage):
        def take(origin):
            from_y, from_x, apart = k_place(origin)
            far = jnp.logical_or(
                jnp.logical_and(from_y == 0, at_y == 2), jnp.logical_and(from_y == 1, at_y == 3)
            )
            hops = jnp.minimum(apart, side_x - apart) + jnp.where(
                from_y == at_y, 0, jnp.where(far, 2, 1)
            )

            def act():
                for half in range(2):
                    k_copy(origin, half, 0).wait_recv()
                k_pass(origin, lambda copy: copy.start())

            guarded(jnp.logical_and(from_y <= at_y, hops == stage), act)

        loop(0, ep_count, take)

    loop(1, ep_count, lambda d: a_copy(d).start())
    recv_a[ep] = outgoing[ep]

    transposed = (((1,), (1,)), ((), ()))
    fetches[1].wait()
    kv_normed = rms_scale(kv_latent_ref[...], kv_gain_ref[...])
    expanded = lax.dot_general(
        w_keyval_ref[...].T, kv_normed, transposed, preferred_element_type=f32
    ).astype(bf16)
    kv[ep, 0:NOPE] = expanded[0:NOPE]
    kv[ep, NOPE:score_rows] = rotate_rows(
        rope_ref[...].astype(f32), cosine_ref[...], sine_ref[...]
    ).astype(bf16)
    kv[ep, score_rows:] = expanded[NOPE:]
    fetches[2].wait()
    q_normed = rms_scale(q_latent_ref[...], q_gain_ref[...])
    projected = lax.dot_general(w_query_ref[...], q_normed, transposed, preferred_element_type=f32)
    queries = jnp.concatenate(
        [
            projected[0:NOPE],
            rotate_rows(projected[NOPE:], cosine_ref[...], sine_ref[...]),
        ],
        0,
    ).astype(bf16)
    for tile in range(tiles):
        q_t[tile] = queries[:, tile * QTILE : (tile + 1) * QTILE]


    def shared_rows(first, count):
        x = layer_scale(
            input_ref[pl.ds(first * count * 2 * MOE_DEV, count * 2 * MOE_DEV), :], gain_ref[...]
        )
        hidden = jax.nn.silu(jnp.dot(x, sgate_ref[...], preferred_element_type=f32))
        hidden = (hidden * jnp.dot(x, sup_ref[...], preferred_element_type=f32)).astype(bf16)
        part = jnp.dot(hidden, sdown_ref[...], preferred_element_type=f32).astype(bf16)
        for at in range(count):
            for side in range(2):
                begin = (at * 2 + side) * MOE_DEV
                buf_p[first * count + at, side, slots:rows, :] = part[begin : begin + MOE_DEV]

    for fetch in fetches[3:7]:
        fetch.wait()
    per_call = 2
    loop(0, z_count // per_call, lambda first: shared_rows(first, per_call))

    m_t[...] = jnp.full_like(m_t, floor_value)
    l_t[...] = jnp.zeros_like(l_t)
    acc_t[...] = jnp.zeros_like(acc_t)

    def squeeze_rows(shape, slot_dim, part=None):
        slot = lax.broadcasted_iota(jnp.int32, shape, slot_dim)
        place = lax.broadcasted_iota(jnp.int32, shape, 1 - slot_dim)
        expert, number = lax.div(slot, CAP), lax.rem(slot, CAP)
        if part is None:
            return jnp.where(place == expert * PAD + number, 1.0, 0.0).astype(bf16)
        target = expert * PAD + CAP + lax.div(number, PACK)
        here = jnp.logical_and(place == target, lax.rem(number, PACK) == part)
        return jnp.where(here, 1.0, 0.0).astype(bf16)

    loop(1, ep_count, lambda d: a_arrival(d).wait_recv())
    arrived = recv_a[...].astype(f32).reshape(ep_count * PAD, PACK * fourth).astype(bf16)
    packed_shape = (slots, ep_count * PAD)
    last = 0.0
    for part in range(PACK):
        piece = arrived[:, columns(part)]
        buf_x[z, core, :, columns(part)] = jnp.dot(
            squeeze_rows(packed_shape, 0), piece, preferred_element_type=f32
        ).astype(bf16)
        last += jnp.dot(squeeze_rows(packed_shape, 0, part), piece, preferred_element_type=f32)
    buf_x[z, core, :, columns(PACK)] = last.astype(bf16)

    def ring_copy(buf, send, recv, size, side, step, half, origin):
        part = pl.ds(half * size, size)
        return remote(
            buf.at[origin, core, part], buf.at[origin, core, part],
            send.at[side, step, half], recv.at[side, step, half], at_z(1 - 2 * side),
        )

    def hand_copy(buf, send, recv, size, offset, half, whose):
        part = pl.ds(half * size, size)
        here = buf.at[around(offset), whose, part]
        return remote(here, here, send.at[offset, half], recv.at[offset, half], partner)

    def x_ring(side, step, half, origin):
        return ring_copy(buf_x, x_send, x_recv, x_half, side, step, half, origin)

    def x_hand(offset, half, whose):
        return hand_copy(buf_x, xd_send, xd_recv, x_half, offset, half, whose)

    def h_ring(side, step, half, origin):
        return ring_copy(heads, h_send, h_recv, h_half, side, step, half, origin)

    def h_hand(offset, half, whose):
        return hand_copy(heads, hd_send, hd_recv, h_half, offset, half, whose)

    def offset_of(side, step):
        return step if side else z_count - step

    def begin_gather(ring, hand):
        for half in range(2):
            for side in range(2):
                ring(side, 1, half, z).start()
            hand(0, half, core).start()

    def pass_on(ring, hand, step):
        for half in range(2):
            for side in range(2):
                offset = offset_of(side, step)
                origin = around(offset)
                ring(side, step, half, origin).wait_recv()
                if half == side:
                    ring(side, step + 1, half, origin).start()
                else:
                    guarded(step < steps, lambda: ring(side, step + 1, half, origin).start())
                hand(offset, half, core).start()

    def pass_last(ring, hand):
        origin = around(half_ring)
        for side in range(2):
            ring(side, half_ring, side, origin).wait_recv()
            hand(half_ring, side, core).start()

    def take_hand(hand, offset):
        for half in range(2):
            hand(offset, half, other).wait_recv()

    def p_copy(offset):
        at = around(offset)
        return remote(buf_p.at[at, other], recv_d.at[at], p_send.at[offset], p_recv.at[offset], partner)

    def expert(offset):
        at = around(offset)
        x = buf_x[at].reshape(2 * slots, width)
        hidden = jax.nn.silu(jnp.dot(x, gate_ref[...], preferred_element_type=f32))
        hidden = (hidden * jnp.dot(x, up_ref[...], preferred_element_type=f32)).astype(bf16)
        part = jnp.dot(hidden, down_ref[...], preferred_element_type=f32).astype(bf16)
        for side in range(2):
            buf_p[at, side, 0:slots, :] = part[side * slots : (side + 1) * slots]
        p_copy(offset).start()

    def pair_sum(offset):
        at = around(offset)
        p_copy(offset).wait_recv()
        for half in range(2):
            for side in range(2):
                part = (slice(half * r_half, (half + 1) * r_half), slice(side * r_cols, (side + 1) * r_cols))
                buf_s[at, side, half] = (
                    buf_p[(at, core) + part].astype(f32) + recv_d[(at,) + part].astype(f32)
                ).astype(bf16)

    def visit(block, tile, key_count, masked):
        scores = lax.dot_general(
            block[0:score_rows, 0:key_count],
            q_t[tile],
            (((0,), (0,)), ((), ())),
            preferred_element_type=f32,
        )
        if masked:
            key_at = lax.broadcasted_iota(jnp.int32, scores.shape, 0)
            query_at = tile * QTILE + lax.broadcasted_iota(jnp.int32, scores.shape, 1)
            scores = jnp.where(key_at <= query_at, scores, floor_value)
        old_max = m_t[tile]
        new_max = jnp.maximum(old_max, jnp.max(scores, 0, keepdims=True))
        weights = jnp.exp2((scores - new_max) * scale)
        fade = jnp.exp2((old_max - new_max) * scale)
        l_t[tile] = l_t[tile] * fade + jnp.sum(weights, 0, keepdims=True)
        attended = jnp.dot(
            block[score_rows:, 0:key_count], weights.astype(bf16), preferred_element_type=f32
        )
        acc_t[tile] = acc_t[tile] * fade + attended
        m_t[tile] = new_max

    def whole_block(origin):
        for tile in range(tiles):
            visit(kv.at[origin], tile, length, False)

    def near_block(which):
        origin = ep - side_x + jnp.where(
            which == 1,
            side_x - 1,
            lax.rem(at_x + jnp.where(which == 2, 3, jnp.where(which == 3, 1, 0)), side_x) - at_x,
        )
        present = jnp.where(which == 1, at_x, at_y) > 0
        guarded(present, lambda: whole_block(origin))

    far_rows = side_x * jnp.maximum(at_y - 1, 0)
    far_count = far_rows + jnp.minimum(at_y, 1) + jnp.maximum(at_x - 1, 0)

    def part_block(unit):
        at = lax.div(unit, 2)
        which = lax.rem(unit, 2)
        row = at_y * side_x
        beside = row - side_x + lax.rem(at_x + 2, side_x)
        after = at - far_rows
        origin = jnp.where(
            after < 0,
            at,
            jnp.where(
                jnp.logical_and(after == 0, at_y > 0), beside, row + after - jnp.minimum(at_y, 1)
            ),
        )
        for tile in range(tiles // 2):
            visit(kv.at[origin], which * (tiles // 2) + tile, length, False)

    begin_gather(x_ring, x_hand)
    k_pass(ep, lambda copy: copy.start())
    for tile in range(tiles):
        visit(kv.at[ep], tile, (tile + 1) * QTILE, True)
    for fetch in fetches[7:10]:
        fetch.wait()

    def hidden_work(offset):
        take_hand(x_hand, offset)
        expert(offset)

    def beside(step, side):
        return lax.rem(step * (2 * side - 1) + z_count, z_count)

    def gather_step(step):
        pass_on(x_ring, x_hand, step)
        loop(0, jnp.minimum(step, 2), lambda side: hidden_work(beside(step - 1, side)))
        guarded(step < 3, lambda: k_stage(step))
        guarded(step > 1, lambda: loop(2 * step - 4, 2 * step - 2, near_block))
        loop(0, jnp.minimum(step - 1, 2), lambda side: pair_sum(beside(step - 2, side)))

    loop(1, half_ring, gather_step)

    def r_copy(step, side, half, chunk):
        return remote(
            buf_s.at[chunk, side, half], recv_r.at[step, side, half],
            r_send.at[step, side, half], r_recv.at[step, side, half], at_z(1 - 2 * side),
        )

    def begin_sums():
        for half in range(2):
            for side in range(2):
                r_copy(0, side, half, around(2 * side - 1)).start()

    if half_ring >= 4:
        begin_sums()
    loop(0, 2, lambda side: hidden_work(beside(half_ring - 1, side)))
    pass_last(x_ring, x_hand)
    if half_ring >= 4:
        k_stage(3)
    else:
        loop(half_ring, 4, k_stage)
    hidden_work(half_ring)
    loop(half_ring - 2, min(half_ring + 3, z_count), pair_sum)
    if half_ring < 4:
        begin_sums()
    if half_ring < 4:
        loop(2 * half_ring - 4, 4, near_block)

    events = 4 * (z_count - 2)
    units = 2 * far_count
    quiet = 4

    def sum_event(event):
        step = lax.div(event, 4) + 1
        side = lax.rem(event, 2)
        half = lax.div(lax.rem(event, 4), 2)
        chunk = around((step + 1) * (2 * side - 1))
        r_copy(step - 1, side, half, chunk).wait_recv()
        buf_s[chunk, side, half] = (
            buf_s[chunk, side, half].astype(f32) + recv_r[step - 1, side, half].astype(f32)
        ).astype(bf16)
        r_copy(step, side, half, chunk).start()
        guarded(event == quiet - 1, lambda: k_stage(4))
        done = jnp.maximum(event - quiet, 0) * units
        due = jnp.maximum(event + 1 - quiet, 0) * units
        loop(lax.div(done, events - quiet), lax.div(due, events - quiet), part_block)

    loop(0, events, sum_event)

    for tile in range(tiles):
        heads[z, core, :, tile * QTILE : (tile + 1) * QTILE] = (acc_t[tile] / l_t[tile]).astype(bf16)
    begin_gather(h_ring, h_hand)

    for half in range(2):
        for side in range(2):
            r_copy(z_count - 2, side, half, z).wait_recv()
            final[half * r_half : (half + 1) * r_half, side * r_cols : (side + 1) * r_cols] = (
                buf_s[z, side, half].astype(f32) + recv_r[z_count - 2, side, half].astype(f32)
            )

    sums = final[0:slots, :].astype(bf16)
    spread_shape = (ep_count * PAD, slots)
    for part in range(PACK):
        spread = jnp.dot(
            squeeze_rows(spread_shape, 1), sums[:, columns(part)], preferred_element_type=f32
        ) + jnp.dot(
            squeeze_rows(spread_shape, 1, part), sums[:, columns(PACK)], preferred_element_type=f32
        )
        send_b[:, :, columns(part)] = spread.reshape(ep_count, PAD, fourth).astype(bf16)

    def b_copy(d):
        there = lax.rem(ep + d, ep_count)
        return remote(send_b.at[there], recv_b.at[ep], b_send.at[d], b_recv.at[d], at_ep(d))

    def b_arrival(d):
        source = lax.rem(ep - d + ep_count, ep_count)
        return remote(send_b.at[ep], recv_b.at[source], b_send.at[d], b_recv.at[d], at_ep(d))

    loop(1, ep_count, lambda d: b_copy(d).start())
    recv_b[ep] = send_b[ep]

    def all_left(ring, hand):
        def left(step):
            for half in range(2):
                for side in range(2):
                    ring(side, step, half, z).wait_send()

        def handed(offset):
            for half in range(2):
                hand(offset, half, core).wait_send()

        loop(1, half_ring, left)
        for side in range(2):
            ring(side, half_ring, side, z).wait_send()
        loop(0, z_count, handed)

    def summed(step):
        for half in range(2):
            for side in range(2):
                r_copy(step, side, half, z).wait_send()

    loop(1, ep_count, lambda d: a_copy(d).wait_send())
    loop(
        0,
        ep_count,
        lambda origin: guarded(
            lax.div(origin, side_x) <= at_y, lambda: k_pass(origin, lambda copy: copy.wait_send())
        ),
    )
    all_left(x_ring, x_hand)
    loop(0, z_count, lambda offset: p_copy(offset).wait_send())
    loop(0, z_count - 1, summed)

    loop(1, half_ring, lambda step: pass_on(h_ring, h_hand, step))
    pass_last(h_ring, h_hand)

    loop(1, ep_count, lambda d: b_arrival(d).wait_recv())
    returned = recv_b[...].astype(f32).reshape(ep_count * PAD, PACK * fourth).astype(bf16)

    def weighed(chosen, rows_in):
        combine = chosen * weight_of
        high = combine.astype(bf16)
        low = (combine - high.astype(f32)).astype(bf16)
        return jnp.dot(high, rows_in, preferred_element_type=f32) + jnp.dot(
            low, rows_in, preferred_element_type=f32
        )

    last = final[slots:rows, columns(PACK)]
    for part in range(PACK):
        piece = returned[:, columns(part)]
        moe_ref[:, columns(part)] = weighed(taken, piece) + final[slots:rows, columns(part)]
        last += weighed(tails[part], piece)
    moe_ref[:, columns(PACK)] = last

    loop(0, z_count, lambda offset: take_hand(h_hand, offset))
    fetches[10].wait()
    mixed_ref[...] = lax.dot_general(
        heads[...].reshape(2 * z_count * VDIM, length),
        wout_ref[...],
        (((0,), (0,)), ((), ())),
        preferred_element_type=f32,
    )

    loop(1, ep_count, lambda d: b_copy(d).wait_send())
    all_left(h_ring, h_hand)


def fused(ep_count, tp_count, width, operands):
    f32, bf16 = jnp.float32, jnp.bfloat16
    z_count = tp_count // 2
    half_ring = z_count // 2
    slots = ep_count * CAP
    rows = slots + MOE_DEV
    score_rows, length = NOPE + ROPE_DIM, operands[2].shape[1]
    staged = operands[HELD:]
    tiles = length // QTILE
    dma = pltpu.SemaphoreType.DMA
    vmem = pltpu.VMEM
    return pl.pallas_call(
        functools.partial(fused_kernel, ep_count, z_count),
        out_shape=(
            jax.ShapeDtypeStruct((length, operands[-1].shape[1]), f32),
            jax.ShapeDtypeStruct((MOE_DEV, width), f32),
        ),
        in_specs=[pl.BlockSpec(memory_space=pltpu.VMEM)] * HELD
        + [pl.BlockSpec(memory_space=pl.ANY)] * len(staged),
        out_specs=(pl.BlockSpec(memory_space=pltpu.VMEM),) * 2,
        scratch_shapes=[
            vmem((MOE_DEV, width), bf16),
            *[vmem(array.shape, bf16) for array in staged],
            dma((len(staged) + 1,)),
            vmem((ep_count, PAD, width // 4 * PACK), bf16),
            vmem((ep_count, PAD, width // 4 * PACK), bf16),
            vmem((z_count, 2, slots, width), bf16),
            vmem((z_count, 2, rows, width), bf16),
            vmem((z_count, rows, width), bf16),
            vmem((z_count, 2, 2, rows // 2, width // 2), bf16),
            vmem((z_count - 1, 2, 2, rows // 2, width // 2), bf16),
            vmem((rows, width), f32),
            vmem((ep_count, score_rows + VDIM, length), bf16),
            vmem((z_count, 2, VDIM, length), bf16),
            vmem((ep_count, PAD, width // 4 * PACK), bf16),
            vmem((ep_count, PAD, width // 4 * PACK), bf16),
            vmem((tiles, score_rows, QTILE), bf16),
            vmem((tiles, 1, QTILE), f32),
            vmem((tiles, 1, QTILE), f32),
            vmem((tiles, VDIM, QTILE), f32),
            dma((ep_count,)),
            dma((ep_count,)),
            dma((ep_count, 2, 4)),
            dma((ep_count, 2)),
            dma((2, half_ring + 1, 2)),
            dma((2, half_ring + 1, 2)),
            dma((z_count, 2)),
            dma((z_count, 2)),
            dma((z_count,)),
            dma((z_count,)),
            dma((z_count - 1, 2, 2)),
            dma((z_count - 1, 2, 2)),
            dma((2, half_ring + 1, 2)),
            dma((2, half_ring + 1, 2)),
            dma((z_count, 2)),
            dma((z_count, 2)),
            dma((ep_count,)),
            dma((ep_count,)),
        ],
        compiler_params=pltpu.CompilerParams(
            collective_id=0, has_side_effects=True, vmem_limit_bytes=62 << 20
        ),
        name="fused",
    )(*operands)


def body(
    q_latent,
    kv_latent,
    rope_key,
    q_gain,
    kv_gain,
    w_query,
    w_keyval,
    w_output,
    moe_input,
    moe_gain,
    routes,
    route_weight,
    expert_gate,
    expert_up,
    expert_down,
    shared_gate,
    shared_up,
    shared_down,
):
    row_count = q_latent.shape[0]
    own_index = lax.axis_index("ep")
    ep_count = lax.axis_size("ep")
    tp_count = lax.axis_size("tp")
    width = moe_input.shape[1]

    positions = own_index * row_count + jnp.arange(row_count, dtype=jnp.int32)
    cosine_table, sine_table = rotary_tables(positions)
    mixed, moe_out = fused(
        ep_count,
        tp_count,
        width,
        (
            cosine_table,
            sine_table,
            rope_key.T,
            q_gain.reshape(1, -1),
            kv_gain.reshape(1, -1),
            moe_gain.reshape(1, -1),
            routes.T,
            route_weight.T,
            w_query.T,
            w_keyval,
            moe_input,
            kv_latent,
            q_latent,
            shared_gate,
            shared_up,
            shared_down,
            expert_gate[0],
            expert_up[0],
            expert_down[0],
            w_output,
        ),
    )
    return (mixed.astype(jnp.bfloat16), moe_out.astype(jnp.bfloat16))


def solution(mesh):
    in_specs = (
        P("ep", None),
        P("ep", None),
        P("ep", None),
        P(),
        P(),
        P(None, "tp"),
        P(None, "tp"),
        P(None, "tp"),
        P("ep", None),
        P(),
        P("ep", None),
        P("ep", None),
        P("ep", None, "tp"),
        P("ep", None, "tp"),
        P("ep", "tp", None),
        P(None, "tp"),
        P(None, "tp"),
        P("tp", None),
    )
    out_specs = (P("ep", "tp"), P(("ep", "tp"), None))
    return jax.shard_map(body, mesh=mesh, in_specs=in_specs, out_specs=out_specs, check_vma=False)
```
